256 devices in a mesh: sp: 64 (over z, x, core), tp: 4 (over y).
Axes of the slice: x: 4, y: 4, z: 8, core: 2. Of those that a mesh axis runs over, the one named last changes fastest.
Arguments:
- mid: bfloat16 [12288, 2048], P('sp'), may hold values from -6 to 6
- out_grad: bfloat16 [12288, 2048], P('sp'), may hold values from -16 to 16
- expert_ids: int32 [12288, 2], P('sp'), may hold values from 0 to 63, all different within a row; in each aligned block of 192 rows (0 to 191, 192 to 383, ...) at most 9 rows name the same one
- route_weights: float32 [12288, 2], P('sp'), may hold values from 0.1 to 0.9
- gate_proj: bfloat16 [64, 2048, 1024], P('sp', None, 'tp'), may hold values from -0.375 to 0.375
- up_proj: bfloat16 [64, 2048, 1024], P('sp', None, 'tp'), may hold values from -0.375 to 0.375
- down_proj: bfloat16 [64, 1024, 2048], P('sp', 'tp'), may hold values from -0.1875 to 0.1875
- out_proj: bfloat16 [512, 2048], P('tp'), may hold values from -0.25 to 0.25
- branch_gate: bfloat16 [12288, 512], P('sp', 'tp'), may hold values from -6 to 6
- conv_out: bfloat16 [2, 12288, 512], P(None, 'sp', 'tp'), may hold values from -6 to 6
- prior_state: float32 [2, 12288, 512], P(None, 'sp', 'tp'), may hold values from -6 to 6
- rate_gate_w: bfloat16 [2, 8, 64, 64], P(None, 'tp'), may hold values from -0.75 to 0.75
- input_gate_w: bfloat16 [2, 8, 64, 64], P(None, 'tp'), may hold values from -0.75 to 0.75
- decay_param: float32 [2, 512], P(None, 'tp'), may hold values from 4 to 16
- decay_jump: float32 [2, 12288, 512], P(None, 'sp', 'tp'), may hold values from -2 to 0
- conv_taps: bfloat16 [2, 4, 512], P(None, None, 'tp'), may hold values from -3 to 3
Outputs:
- gate_grad: bfloat16 [64, 2048, 1024], P('sp', None, 'tp')
- up_grad: bfloat16 [64, 2048, 1024], P('sp', None, 'tp')
- down_grad: bfloat16 [64, 1024, 2048], P('sp', 'tp')
- proj_grad_t: float32 [2048, 512], P('sp', 'tp')
- input_grad: bfloat16 [12288, 512], P('sp', 'tp')
- branch_gate_grad: bfloat16 [12288, 512], P('sp', 'tp')
The draws below stay inside these ranges and needn't reach their ends.
Inputs may be any that keep to these rules, and one draw needn't show every extreme that they name: `expert_ids`: each row names 2 different experts. Among the rows of one device no expert is named by more than 9 rows, a bound that some block reaches of some device.
All inputs are finite; a program needn't handle non-finite values.
Results may differ from the reference program's by a relative error of at most 0.023.
The reference program's roundings to bfloat16 on the way count: a program that leaves them out, or rounds other values in their place, can miss the bound.
Values may be sent and summed in bfloat16 or wider, within the bound.
No kernel may reach another device: no remote copies, remote signals or barrier semaphores. Data moves between devices by JAX's collectives and lax.ppermute only.
A program may use at most 64 MiB of HBM per device.

```python
import math
import jax
import jax.numpy as jnp
import numpy as np
from jax import lax

D = 2048
FF = 1024
HEADS = 8
HEAD = 64
W = 512
TAPS = 4
TOP = 2
EXPERTS = 64
TOK_DEV = 192
CAP = 9
STREAM_ITEMS = 12288
N_SP = 64
N_TP = 4


def draw_decay_param(key, part):
    selection_seed, slow_key, fast_key = jax.random.split(jax.random.fold_in(key, 11), 3)
    slow_share = 0.5
    slow_mask = jax.random.uniform(selection_seed, (2, W), jnp.float32) < slow_share
    slow_rate = jnp.exp(jax.random.uniform(slow_key, (2, W), jnp.float32, jnp.log(0.02), jnp.log(0.12))) / STREAM_ITEMS
    fast_rate = jnp.exp(jax.random.uniform(fast_key, (2, W), jnp.float32, jnp.log(0.0025), jnp.log(0.008)))
    rates = jnp.where(slow_mask, slow_rate, fast_rate)
    return -jnp.log(jnp.expm1(rates))


def draw_decay_jump(key, part):
    block_key, place_key, loss_key = jax.random.split(jax.random.fold_in(key, 23), 3)
    block_count = STREAM_ITEMS // TOK_DEV
    factors = jnp.exp(jax.random.uniform(block_key, (2, block_count, 1), jnp.float32, jnp.log(0.1), jnp.log(0.8)))
    equilibrium_level = -jnp.repeat(factors, TOK_DEV, axis=1) / STREAM_ITEMS
    assigned_positions = jax.random.randint(place_key, (2, 2), 0, STREAM_ITEMS)
    objective_scores = jax.random.uniform(loss_key, (2, 2, W), jnp.float32, 0.2, 0.5)
    arrival_tallies = (jnp.arange(STREAM_ITEMS, dtype=jnp.int32)[None, :, None] == assigned_positions[:, None, :]).astype(jnp.float32)
    return equilibrium_level + jnp.einsum('dwp,dpu->dwu', arrival_tallies, jnp.log1p(-objective_scores))


def spiked(drawn, key, source, target, parts, factor):
    owner, partner = [(jnp.arange(drawn.shape[axis_at]) // (drawn.shape[axis_at] // parts)).reshape([-1 if axis == axis_at else 1 for axis in range(drawn.ndim)]) for axis_at in (source, target)]
    chosen = jax.random.permutation(key, parts)[partner]
    strong = (owner == chosen) | (owner == (partner + parts // 2) % parts)
    return jnp.where(strong, factor * drawn, drawn)


def steps_of(key, extent, cuts, least, top_value):
    def one(axis_at, blocks):
        draws = jax.random.uniform(jax.random.fold_in(jax.random.fold_in(key, 6), axis_at), (blocks,), jnp.float32, least / len(cuts), top_value / len(cuts))
        return jnp.repeat(jnp.exp(draws), extent[axis_at] // blocks).reshape((-1,) + (1,) * (len(extent) - axis_at - 1))

    loudness = one(*cuts[0])
    for cut in cuts[1:]:
        loudness = loudness * one(*cut)
    return loudness


def routed_block(stream_key, own, number, rows, count, top, limit, slope):
    ranking = jax.random.permutation(stream_key, count)
    packed, usual = shares(count, rows * top, limit, slope, True), shares(count, rows * top, limit, slope, False)
    places = jnp.arange(count)

    def named(tallies, turn):
        used = int((tallies > 0).sum())
        fixed = max(1, used // 4)
        shifted = fixed + (places - fixed + turn * (used - fixed)) % max(1, count - fixed)
        return jnp.zeros((count,), jnp.int32).at[ranking[jnp.where(places < fixed, places, shifted)]].set(jnp.asarray(tallies, jnp.int32))

    tallies = jnp.where(number % 4 == 0, named(packed, number // 4), named(usual, number - number // 4 - 1))
    mixed = jax.random.permutation(jax.random.fold_in(own, 3), count)
    giver, sink = mixed[0:count // 2 * 2:2], mixed[1:count // 2 * 2:2]
    slack = jnp.minimum(tallies[giver] - 1, limit - tallies[sink]) // 2
    slack = jnp.where((giver == ranking[0]) | (sink == ranking[0]) | (tallies[sink] == 0), 0, jnp.maximum(slack, 0))
    shifted = jax.random.randint(jax.random.fold_in(own, 4), (count // 2,), 0, 1 << 20) % (slack + 1)
    tallies = tallies.at[giver].add(-shifted).at[sink].add(shifted)
    labels = jnp.searchsorted(jnp.cumsum(tallies), jnp.arange(rows * top), side="right").astype(jnp.int32)
    listing = labels.reshape(top, rows).T
    listing = listing[jax.random.permutation(jax.random.fold_in(own, 1), rows)]
    turn = jax.random.randint(jax.random.fold_in(own, 2), (rows, 1), 0, top)
    return jnp.take_along_axis(listing, (jnp.arange(top)[None, :] + turn) % top, axis=1)


def shares(number_of, total, bound, skew, full):
    weights = [(1 << 20) // math.isqrt(rank ** skew) + 1 for rank in range(1, number_of + 1)]
    largest = bound if full else min(bound, max(-(-total // number_of), total * weights[0] // sum(weights)))
    least = 1 if total - largest >= number_of - 1 else 0
    given, surplus = [largest] + [least] * (number_of - 1), total - largest - least * (number_of - 1)
    while surplus > 0:
        candidates = [i for i in range(1, number_of) if given[i] < largest] or [i for i in range(1, number_of) if given[i] < bound]
        pool, left = sum([weights[i] for i in candidates]), surplus
        for i in candidates:
            more = min(bound - given[i], max(1, left * weights[i] // pool), surplus)
            given[i] = given[i] + more
            surplus = surplus - more
    return np.array(given)


def normal_values(rng, extent, width, most, shards=(), held_as=jnp.bfloat16):
    loudness = steps_of(rng, extent, shards, -0.22, 0.18) if shards else 1.0
    entries = jax.random.normal(rng, extent, jnp.float32) * width * loudness
    return jnp.minimum(jnp.maximum(entries, -most), most).astype(held_as)


def heavy_noise(rng, dims, width, most, cuts, heavy, kind=jnp.bfloat16):
    values = width * jax.random.normal(rng, dims, jnp.float32)
    if cuts:
        values = values * steps_of(rng, dims, cuts, -0.22, 0.18)
    return jnp.clip(spiked(values, jax.random.fold_in(rng, 3), *heavy), -most, most).astype(kind)


def setup_inputs(seed: int = 0) -> dict:
    keys = jax.random.split(jax.random.key(seed), 17)
    mid = normal_values(keys[0], (STREAM_ITEMS, D), 1.0, 6.0, ((0, 64),))
    out_grad = heavy_noise(keys[1], (STREAM_ITEMS, D), 1.0, 16.0, ((0, 64),), (0, 1, 64, 4.0))
    expert_ids_keys = jax.random.split(jax.random.fold_in(keys[2], 1), STREAM_ITEMS // TOK_DEV)
    expert_ids_turns = jax.random.permutation(jax.random.fold_in(keys[2], 3), STREAM_ITEMS // TOK_DEV)
    expert_ids = jax.vmap(lambda own, number: routed_block(jax.random.fold_in(keys[2], 2), own, number, TOK_DEV, EXPERTS, TOP, CAP, 1))(expert_ids_keys, expert_ids_turns).reshape((STREAM_ITEMS, TOP))
    route_weights = jnp.clip(0.1 + 0.79999997 * jax.random.uniform(keys[3], (STREAM_ITEMS, TOP), jnp.float32) ** steps_of(keys[3], (STREAM_ITEMS, TOP), ((0, 64),), -0.2, 0.2), 0.1, 0.9)
    gate_proj = normal_values(keys[4], (EXPERTS, D, FF), (D // 9) ** -0.5, 0.375, ((0, 64), (2, 4)))
    up_proj = normal_values(keys[5], (EXPERTS, D, FF), (D // 9) ** -0.5, 0.375, ((0, 64), (2, 4)))
    down_proj = normal_values(keys[6], (EXPERTS, FF, D), FF ** -0.5, 0.1875, ((0, 64), (1, 4)))
    out_proj = normal_values(keys[7], (W, D), W ** -0.5, 0.25, ((0, 4),))
    branch_gate = normal_values(keys[8], (STREAM_ITEMS, W), 1.0, 6.0, ((0, 64), (1, 4)))
    conv_out = normal_values(keys[9], (2, STREAM_ITEMS, W), 1.0, 6.0, ((1, 64), (2, 4)))
    prior_state = normal_values(keys[10], (2, STREAM_ITEMS, W), 1.0, 6.0, ((1, 64), (2, 4)), jnp.float32)
    rate_gate_w = normal_values(keys[11], (2, HEADS, HEAD, HEAD), HEAD ** -0.5, 0.75, ((1, 4),))
    input_gate_w = normal_values(keys[12], (2, HEADS, HEAD, HEAD), HEAD ** -0.5, 0.75, ((1, 4),))
    decay_param = draw_decay_param(jax.random.fold_in(keys[16], 71), 0)
    decay_jump = draw_decay_jump(jax.random.fold_in(keys[16], 71), 0)
    conv_taps = normal_values(keys[15], (2, TAPS, W), 0.5, 3.0, ((2, 4),))
    return {"mid": mid, "out_grad": out_grad, "expert_ids": expert_ids, "route_weights": route_weights, "gate_proj": gate_proj, "up_proj": up_proj, "down_proj": down_proj, "out_proj": out_proj, "branch_gate": branch_gate, "conv_out": conv_out, "prior_state": prior_state, "rate_gate_w": rate_gate_w, "input_gate_w": input_gate_w, "decay_param": decay_param, "decay_jump": decay_jump, "conv_taps": conv_taps}


RATE_SCALE = 8.0
CLAMP_LIMIT = 7.0
SHARPNESS = 1.702
NORM_EPSILON = 1e-06
STATE_FLOOR = 0.001
GELU_CUBIC = 0.044715
GELU_SCALE = 0.7978845608028654

def gelu_parts(values):
    inside = GELU_SCALE * (values + GELU_CUBIC * values * values * values)
    tangent = jnp.tanh(inside)
    result = 0.5 * values * (1.0 + tangent)
    slope_value = 0.5 * (1.0 + tangent) + 0.5 * values * (1.0 - tangent * tangent) * GELU_SCALE * (1.0 + 3.0 * GELU_CUBIC * values * values)
    return (result, slope_value)

def adjoint_chain(decay_factors, seeds, backward):

    def advance(incoming, step_pair):
        adjoint_now = step_pair[1] + incoming
        return (step_pair[0] * adjoint_now, adjoint_now)
    start_carry = jnp.zeros(seeds.shape[1:], jnp.float32)
    _, totals = lax.scan(advance, start_carry, (decay_factors, seeds), reverse=backward)
    return totals

def reference(mid, out_grad, expert_ids, route_weights, gate_proj, up_proj, down_proj, out_proj, branch_gate, conv_out, prior_state, rate_gate_w, input_gate_w, decay_param, decay_jump, conv_taps):
    mid_full = mid.astype(jnp.float32)
    inv_rms = lax.rsqrt(lax.optimization_barrier(jnp.mean(mid_full * mid_full, axis=1, keepdims=True)) + NORM_EPSILON)
    normed = mid_full * inv_rms
    normed_b = normed.astype(jnp.bfloat16)
    block_ids = expert_ids.reshape(N_SP, TOK_DEV * TOP)
    onehot = (block_ids[:, :, None] == jnp.arange(EXPERTS, dtype=jnp.int32)[None, None, :]).astype(jnp.int32)
    rank_ids = lax.optimization_barrier(jnp.sum((jnp.cumsum(onehot, axis=1) - onehot) * onehot, axis=2))
    positions = (jnp.arange(N_SP, dtype=jnp.int32)[:, None] * CAP + rank_ids).reshape(-1)
    flat_ids = expert_ids.reshape(-1)
    slot_table = jnp.full((EXPERTS, N_SP * CAP), -1, jnp.int32).at[flat_ids, positions].set(jnp.arange(STREAM_ITEMS * TOP, dtype=jnp.int32))
    route_flat = route_weights.reshape(-1)
    ff_group = FF // N_TP

    def expert_step(running, inputs):
        slot_rows, w_gate, w_up, down_weight = inputs
        filled = slot_rows >= 0
        assign = jnp.where(filled, slot_rows, 0)
        token_ids = assign // TOP
        rows_b = jnp.where(filled[:, None], normed_b[token_ids], jnp.zeros((), jnp.bfloat16))
        weights = jnp.where(filled, route_flat[assign], 0.0)
        grad_b = (out_grad[token_ids].astype(jnp.float32) * weights[:, None]).astype(jnp.bfloat16)
        gate_pre = jnp.dot(rows_b, w_gate, preferred_element_type=jnp.float32)
        up_pre = jnp.dot(rows_b, w_up, preferred_element_type=jnp.float32)
        gate_clamped = jnp.minimum(gate_pre, CLAMP_LIMIT)
        up_clamped = jnp.clip(up_pre, -CLAMP_LIMIT, CLAMP_LIMIT)
        gate_sigmoid = jax.nn.sigmoid(SHARPNESS * gate_clamped)
        swish_value = gate_clamped * gate_sigmoid
        act_b = ((up_clamped + 1.0) * swish_value).astype(jnp.bfloat16)
        act_grad = jnp.dot(grad_b, down_weight.T, preferred_element_type=jnp.float32)
        gate_delta = jnp.where(gate_pre < CLAMP_LIMIT, act_grad * (up_clamped + 1.0) * (gate_sigmoid + SHARPNESS * swish_value * (1.0 - gate_sigmoid)), 0.0).astype(jnp.bfloat16)
        up_delta = jnp.where(jnp.abs(up_pre) < CLAMP_LIMIT, act_grad * swish_value, 0.0).astype(jnp.bfloat16)
        down_grad = jnp.dot(act_b.T, grad_b, preferred_element_type=jnp.float32).astype(jnp.bfloat16)
        gate_grad = jnp.dot(rows_b.T, gate_delta, preferred_element_type=jnp.float32).astype(jnp.bfloat16)
        up_grad = jnp.dot(rows_b.T, up_delta, preferred_element_type=jnp.float32).astype(jnp.bfloat16)
        gate_parts = gate_delta.astype(jnp.float32).reshape(-1, N_TP, ff_group)
        up_parts = up_delta.astype(jnp.float32).reshape(-1, N_TP, ff_group)
        gate_cols = w_gate.astype(jnp.float32).reshape(D, N_TP, ff_group)
        up_cols = w_up.astype(jnp.float32).reshape(D, N_TP, ff_group)
        partials = jnp.einsum('rjf,djf->jrd', gate_parts, gate_cols) + jnp.einsum('rjf,djf->jrd', up_parts, up_cols)
        rounded = lax.optimization_barrier(partials.astype(jnp.bfloat16))
        slot_b = lax.optimization_barrier(jnp.sum(rounded.astype(jnp.float32), axis=0)).astype(jnp.bfloat16)
        running = running.at[token_ids].add(jnp.where(filled[:, None], slot_b.astype(jnp.float32), 0.0))
        return (running, (gate_grad, up_grad, down_grad))
    token_grad, (gate_grads, up_grads, down_grads) = lax.scan(expert_step, jnp.zeros((STREAM_ITEMS, D), jnp.float32), (slot_table, gate_proj, up_proj, down_proj))
    inner_mean = lax.optimization_barrier(jnp.mean(token_grad * normed, axis=1, keepdims=True))
    mid_grad_b = (out_grad.astype(jnp.float32) + inv_rms * (token_grad - normed * inner_mean)).astype(jnp.bfloat16)
    branch_grad = jnp.dot(mid_grad_b, out_proj.T, preferred_element_type=jnp.float32)
    conv_full = conv_out.astype(jnp.float32)
    conv_heads = conv_full.reshape(2, STREAM_ITEMS, HEADS, HEAD)
    rate_gate = jax.nn.sigmoid(jnp.einsum('sthc,shcd->sthd', conv_heads, rate_gate_w.astype(jnp.float32)).reshape(2, STREAM_ITEMS, W))
    input_gate = jax.nn.sigmoid(jnp.einsum('sthc,shcd->sthd', conv_heads, input_gate_w.astype(jnp.float32)).reshape(2, STREAM_ITEMS, W))
    decay_rate = jax.nn.softplus(-decay_param)[:, None, :]
    log_decay = -RATE_SCALE * rate_gate * decay_rate + decay_jump
    decay_factors = jnp.exp(log_decay)
    squared = jnp.exp(2.0 * log_decay)
    norm_factor = jnp.sqrt(STATE_FLOOR - jnp.expm1(2.0 * log_decay))
    drive_term = input_gate * conv_full
    states = decay_factors * prior_state + norm_factor * drive_term
    summed_states = states[0] + states[1]
    gelu_value, gelu_slope = gelu_parts(branch_gate.astype(jnp.float32))
    mixed_b = (summed_states * gelu_value).astype(jnp.bfloat16)
    branch_gate_grad = (branch_grad * summed_states * gelu_slope).astype(jnp.bfloat16)
    state_grad = branch_grad * gelu_value
    adjoint = jnp.stack([adjoint_chain(decay_factors[0], state_grad, True), adjoint_chain(decay_factors[1], state_grad, False)])
    decay_grad = adjoint * (decay_factors * prior_state - drive_term * squared / norm_factor)
    drive_grad = adjoint * norm_factor
    rate_pre = (decay_grad * (-RATE_SCALE * decay_rate) * rate_gate * (1.0 - rate_gate)).astype(jnp.bfloat16)
    input_pre = (drive_grad * conv_full * input_gate * (1.0 - input_gate)).astype(jnp.bfloat16)
    conv_grad = drive_grad * input_gate
    conv_grad = conv_grad + jnp.einsum('sthd,shcd->sthc', rate_pre.astype(jnp.float32).reshape(2, STREAM_ITEMS, HEADS, HEAD), rate_gate_w.astype(jnp.float32)).reshape(2, STREAM_ITEMS, W)
    conv_grad = conv_grad + jnp.einsum('sthd,shcd->sthc', input_pre.astype(jnp.float32).reshape(2, STREAM_ITEMS, HEADS, HEAD), input_gate_w.astype(jnp.float32)).reshape(2, STREAM_ITEMS, W)
    reach = TAPS - 1
    padded = jnp.pad(conv_grad, ((0, 0), (reach, reach), (0, 0)))
    taps_full = conv_taps.astype(jnp.float32)
    input_grad = jnp.zeros((STREAM_ITEMS, W), jnp.float32)
    for tap_index in range(TAPS):
        upper = 2 * reach - tap_index
        input_grad = input_grad + taps_full[0, tap_index] * padded[0, upper:upper + STREAM_ITEMS] + taps_full[1, tap_index] * padded[1, tap_index:tap_index + STREAM_ITEMS]
    proj_grad_t = jnp.dot(mid_grad_b.T, mixed_b, preferred_element_type=jnp.float32)
    return (gate_grads, up_grads, down_grads, proj_grad_t, input_grad.astype(jnp.bfloat16), branch_gate_grad)
```

```python
import jax
import jax.numpy as jnp
from jax import lax
from jax.sharding import PartitionSpec as P

RATE_SCALE = 8.0
CLAMP_LIMIT = 7.0
SHARPNESS = 1.702
NORM_EPSILON = 1e-06
STATE_FLOOR = 0.001
GELU_CUBIC = 0.044715
GELU_SCALE = 0.7978845608028654
LANES = 128


def in_one_piece(arrays, axis, split_dim, concat_dim, along):
    ends, at = ([], 0)
    for a in arrays[:-1]:
        at += a.shape[along]
        ends.append(at)
    both = jnp.concatenate(arrays, axis=along)
    return tuple(
        jnp.split(
            lax.all_to_all(both, axis, split_axis=split_dim, concat_axis=concat_dim, tiled=True),
            ends,
            axis=along,
        )
    )


def side_by_side(arrays, axis, dim, along):
    widths = [a.shape[along] for a in arrays]
    both = jnp.concatenate(arrays, axis=along)
    out = lax.all_gather(both, axis, axis=dim, tiled=True)
    return tuple(jnp.split(out, [sum(widths[:k]) for k in range(1, len(widths))], axis=along))


def in_blocks(x, dim, count):
    dims = x.shape
    tiles = x.reshape(*dims[:dim], count, dims[dim] // count, *dims[dim + 1 :])
    return jnp.moveaxis(tiles, dim, 0)


def summed_on_arrival(x, axis, dim):
    tiles = in_blocks(x, dim, lax.axis_size(axis))
    arrived = lax.all_to_all(tiles, axis, split_axis=0, concat_axis=0, tiled=True)
    return arrived.astype(jnp.float32).sum(axis=0)


def ring_pairs(axis):
    count = lax.axis_size(axis)
    forward = [(i, (i + 1) % count) for i in range(count)]
    return forward, [(target, source) for source, target in forward]


def ring_blocks(x, axis):
    forward, backward = ring_pairs(axis)
    half = x.shape[0] // 2
    left = lax.ppermute(x, axis, forward)
    right = lax.ppermute(x, axis, backward)
    far_top = lax.ppermute(left[:half], axis, forward)
    far_bottom = lax.ppermute(right[half:], axis, backward)
    return x, right, jnp.concatenate([far_top, far_bottom], axis=0), left


def ring_sum(partial, half, axis):
    forward, backward = ring_pairs(axis)
    far = partial(2).astype(jnp.bfloat16)
    from_left = lax.ppermute(far[:half], axis, forward).astype(jnp.float32)
    from_right = lax.ppermute(far[half:], axis, backward).astype(jnp.float32)
    to_right, to_left = partial(1), partial(3)
    to_right = jnp.concatenate([to_right[:half] + from_left, to_right[half:]])
    to_left = jnp.concatenate([to_left[:half], to_left[half:] + from_right])
    got_left = lax.ppermute(to_right.astype(jnp.bfloat16), axis, forward)
    got_right = lax.ppermute(to_left.astype(jnp.bfloat16), axis, backward)
    return partial(0) + got_left.astype(jnp.float32) + got_right.astype(jnp.float32)


def laid_out(tiles, dim):
    tiles = jnp.moveaxis(tiles, 0, dim)
    dims = tiles.shape
    return tiles.reshape(*dims[:dim], dims[dim] * dims[dim + 1], *dims[dim + 2 :])


def sent_to_all(x, axis):
    copies = jnp.broadcast_to(x, (lax.axis_size(axis), *x.shape))
    return lax.all_to_all(copies, axis, split_axis=0, concat_axis=0, tiled=True)


def gathered_copies(x, axis, dim):
    return laid_out(sent_to_all(x, axis), dim)


def collected_together(x, axis):
    leaves = jax.tree.leaves(x)
    order = sorted(range(len(leaves)), key=lambda k: -leaves[k].size)
    width = (1, *leaves[order[0]].shape)[-1]
    lines = [
        jnp.pad(leaves[k].reshape(-1), (0, -leaves[k].size % width)).reshape(-1, width)
        for k in order
    ]
    both, at, found = (sent_to_all(jnp.concatenate(lines), axis), 0, {})
    for k, line in zip(order, lines):
        piece = both[:, at : at + len(line)].reshape(len(both), -1)
        found[k] = piece[:, : leaves[k].size].reshape(-1, *leaves[k].shape)
        at += len(line)
    numbers = iter(range(len(leaves)))
    return jax.tree.map(lambda _: found[next(numbers)], x)


def joined_by_halves(pieces, combine):
    while len(jax.tree.leaves(pieces)[0]) > 1:
        pieces = jax.vmap(combine)(
            *(jax.tree.map(lambda part: part[side::2], pieces) for side in (0, 1))
        )
    return jax.tree.map(lambda part: part[0], pieces)


def entering(x, axis, combine, identity, reverse):
    count, place = (lax.axis_size(axis), lax.axis_index(axis))
    passed = jnp.arange(count) > place if reverse else jnp.arange(count) < place

    def kept(part, zero, own):
        part = jnp.where(
            passed.reshape(-1, *(1 for _ in own.shape)), part, jnp.asarray(zero, own.dtype)
        )
        return part[::-1] if reverse else part

    pieces = collected_together(x, axis)
    return joined_by_halves(jax.tree.map(kept, pieces, identity, x), combine)


def shortened(x):
    return jax.tree.map(lambda a: a.astype(jnp.bfloat16) if a.dtype == jnp.float32 else a, x)


def with_halo(block, sides, width):
    for axis, dim in sides:
        count = lax.axis_size(axis)
        forward = [(i, i + 1) for i in range(count - 1)]
        backward = [(target, source) for source, target in forward]
        low = lax.ppermute(
            lax.slice_in_dim(block, block.shape[dim] - width, None, axis=dim), axis, forward
        )
        high = lax.ppermute(lax.slice_in_dim(block, 0, width, axis=dim), axis, backward)
        block = jnp.concatenate([low, block, high], axis=dim)
    return block


def gelu_parts(values):
    inside = GELU_SCALE * (values + GELU_CUBIC * values * values * values)
    tangent = jnp.tanh(inside)
    result = 0.5 * values * (1.0 + tangent)
    slope_value = 0.5 * (1.0 + tangent) + 0.5 * values * (1.0 - tangent * tangent) * GELU_SCALE * (
        1.0 + 3.0 * GELU_CUBIC * values * values
    )
    return (result, slope_value)


def chain_scan(factors, seeds):

    def link_pairs(first_pair, second_pair):
        return (first_pair[0] * second_pair[0], second_pair[0] * first_pair[1] + second_pair[1])

    return lax.associative_scan(link_pairs, (factors, seeds), axis=0)


def compose(former, latter):
    return (latter[0] * former[0], latter[0] * former[1] + latter[1])


def on_device(
    mid,
    out_grad,
    expert_ids,
    route_weights,
    gate_proj,
    up_proj,
    down_proj,
    out_proj,
    branch_gate,
    conv_out,
    prior_state,
    rate_gate_w,
    input_gate_w,
    decay_param,
    decay_jump,
    conv_taps,
):
    tok_rows, embedding_width = mid.shape
    shards = lax.axis_size("sp")
    groups = lax.axis_size("tp")
    local_experts = gate_proj.shape[0]
    experts_all = local_experts * shards
    top_count = expert_ids.shape[1]
    expert_room = 3 * top_count * tok_rows // (2 * experts_all)
    slot_count = experts_all * expert_room
    mid_full = mid.astype(jnp.float32)
    inv_rms = lax.rsqrt(jnp.mean(mid_full * mid_full, axis=1, keepdims=True) + NORM_EPSILON)
    normed = mid_full * inv_rms
    normed_b = normed.astype(jnp.bfloat16)
    flat_ids = expert_ids.reshape(-1)
    onehot = (flat_ids[:, None] == jnp.arange(experts_all, dtype=jnp.int32)[None, :]).astype(
        jnp.int32
    )
    rank_ids = jnp.sum((jnp.cumsum(onehot, axis=0) - onehot) * onehot, axis=1)
    slot_ids = (flat_ids * expert_room + rank_ids).reshape(tok_rows, top_count)
    matches = slot_ids[None, :, :] == jnp.arange(slot_count, dtype=jnp.int32)[:, None, None]
    select = jnp.any(matches, axis=2).astype(jnp.bfloat16)
    slot_gate = jnp.sum(jnp.where(matches, route_weights[None, :, :], 0.0), axis=(1, 2))
    place = lax.axis_index("tp")
    span = embedding_width // groups

    def packed(x):
        return x.reshape(shards, -1, LANES)

    def turned(x, dim):
        return jnp.concatenate(
            [
                lax.dynamic_slice_in_dim(x, ((place + k) % groups) * span, span, dim)
                for k in range(groups)
            ],
            axis=dim,
        )

    rows_source = lax.dynamic_slice_in_dim(normed_b, place * span, span, 1)
    grad_source = lax.dynamic_slice_in_dim(out_grad, place * span, span, 1)
    sent_rows = jnp.dot(select, rows_source, preferred_element_type=jnp.float32).astype(
        jnp.bfloat16
    )
    sent_grad = (
        jnp.dot(select, grad_source, preferred_element_type=jnp.float32) * slot_gate[:, None]
    ).astype(jnp.bfloat16)
    got_rows = lax.all_to_all(packed(sent_rows), "sp", 0, 0, tiled=True).reshape(slot_count, span)
    got_grad = lax.all_to_all(packed(sent_grad), "sp", 0, 0, tiled=True).reshape(slot_count, span)
    rows = ring_blocks(got_rows, "tp")
    grads = ring_blocks(got_grad, "tp")
    both_proj = jnp.concatenate([turned(gate_proj[0], 0), turned(up_proj[0], 0)], axis=1)
    down_turned = turned(down_proj[0], 1)
    hidden = gate_proj.shape[2]
    pre = sum(
        jnp.dot(
            rows[k], both_proj[k * span : (k + 1) * span], preferred_element_type=jnp.float32
        )
        for k in range(groups)
    )
    gate_pre, up_pre = pre[:, :hidden], pre[:, hidden:]
    gate_clamped = jnp.minimum(gate_pre, CLAMP_LIMIT)
    up_clamped = jnp.clip(up_pre, -CLAMP_LIMIT, CLAMP_LIMIT)
    gate_sigmoid = jax.nn.sigmoid(SHARPNESS * gate_clamped)
    swish_value = gate_clamped * gate_sigmoid
    act_b = ((up_clamped + 1.0) * swish_value).astype(jnp.bfloat16)
    act_grad = sum(
        jnp.einsum(
            "rd,fd->rf",
            grads[k],
            down_turned[:, k * span : (k + 1) * span],
            preferred_element_type=jnp.float32,
        )
        for k in range(groups)
    )
    gate_delta = jnp.where(
        gate_pre < CLAMP_LIMIT,
        act_grad
        * (up_clamped + 1.0)
        * (gate_sigmoid + SHARPNESS * swish_value * (1.0 - gate_sigmoid)),
        0.0,
    ).astype(jnp.bfloat16)
    up_delta = jnp.where(jnp.abs(up_pre) < CLAMP_LIMIT, act_grad * swish_value, 0.0).astype(
        jnp.bfloat16
    )
    deltas = jnp.concatenate([gate_delta, up_delta], axis=1)

    def partial(k):
        return jnp.einsum(
            "rf,df->rd",
            deltas,
            both_proj[k * span : (k + 1) * span],
            preferred_element_type=jnp.float32,
        )

    summed = ring_sum(partial, slot_count // 2, "tp")
    returned = lax.all_to_all(packed(summed.astype(jnp.bfloat16)), "sp", 0, 0, tiled=True).reshape(
        slot_count, span
    )

    def in_order(blocks):
        stack = jnp.stack(blocks)
        return jnp.concatenate(
            [
                lax.dynamic_index_in_dim(stack, (k - place) % groups, 0, keepdims=False)
                for k in range(groups)
            ],
            axis=1,
        )

    expert_rows, expert_grads, deltas_late, act_late = lax.optimization_barrier(
        (in_order(rows), in_order(grads), deltas, act_b)
    )
    down_grad = jnp.einsum(
        "rf,rd->fd", act_late, expert_grads, preferred_element_type=jnp.float32
    ).astype(jnp.bfloat16)[None]
    gate_grad = jnp.einsum(
        "rd,rf->df", expert_rows, deltas_late[:, :hidden], preferred_element_type=jnp.float32
    ).astype(jnp.bfloat16)[None]
    up_grad = jnp.einsum(
        "rd,rf->df", expert_rows, deltas_late[:, hidden:], preferred_element_type=jnp.float32
    ).astype(jnp.bfloat16)[None]
    token_grad = jnp.einsum("st,sd->td", select, returned, preferred_element_type=jnp.float32)
    token_grad = gathered_copies(token_grad.astype(jnp.bfloat16), "tp", 1).astype(token_grad.dtype)
    inner_mean = jnp.mean(token_grad * normed, axis=1, keepdims=True)
    mid_grad_b = (
        out_grad.astype(jnp.float32) + inv_rms * (token_grad - normed * inner_mean)
    ).astype(jnp.bfloat16)
    heads_local = rate_gate_w.shape[1]
    head_width = rate_gate_w.shape[2]
    channels = heads_local * head_width
    branch_grad = jnp.einsum("td,cd->tc", mid_grad_b, out_proj, preferred_element_type=jnp.float32)
    conv_heads = conv_out.reshape(2, tok_rows, heads_local, head_width)
    rate_gate = jax.nn.sigmoid(
        jnp.einsum(
            "sthc,shcd->sthd", conv_heads, rate_gate_w, preferred_element_type=jnp.float32
        ).reshape(2, tok_rows, channels)
    )
    input_gate = jax.nn.sigmoid(
        jnp.einsum(
            "sthc,shcd->sthd", conv_heads, input_gate_w, preferred_element_type=jnp.float32
        ).reshape(2, tok_rows, channels)
    )
    decay_rate = jax.nn.softplus(-decay_param)[:, None, :]
    log_decay = -RATE_SCALE * rate_gate * decay_rate + decay_jump
    decay_factors = jnp.exp(log_decay)
    squared = jnp.exp(2.0 * log_decay)
    norm_factor = jnp.sqrt(STATE_FLOOR - jnp.expm1(2.0 * log_decay))
    conv_full = conv_out.astype(jnp.float32)
    drive_term = input_gate * conv_full
    states = decay_factors * prior_state + norm_factor * drive_term
    summed_states = states[0] + states[1]
    gelu_value, gelu_slope = gelu_parts(branch_gate.astype(jnp.float32))
    mixed_b = (summed_states * gelu_value).astype(jnp.bfloat16)
    branch_gate_grad = (branch_grad * summed_states * gelu_slope).astype(jnp.bfloat16)
    state_grad = branch_grad * gelu_value
    ones_row = jnp.ones((1, channels), jnp.float32)
    later_factors = jnp.concatenate([decay_factors[0, 1:], ones_row], axis=0)
    later_prod, later_local = chain_scan(jnp.flip(later_factors, 0), jnp.flip(state_grad, 0))
    later_prod = jnp.flip(later_prod, 0)
    later_local = jnp.flip(later_local, 0)
    earlier_factors = jnp.concatenate([ones_row, decay_factors[1, :-1]], axis=0)
    earlier_prod, earlier_local = chain_scan(earlier_factors, state_grad)
    later_map = (decay_factors[0, 0] * later_prod[0], decay_factors[0, 0] * later_local[0])
    earlier_map = (
        decay_factors[1, -1] * earlier_prod[-1],
        decay_factors[1, -1] * earlier_local[-1],
    )
    maps = sent_to_all(jnp.stack([*later_map, *earlier_map]), "sp")
    count, here = (lax.axis_size("sp"), lax.axis_index("sp"))
    at = jnp.arange(count)[:, None]

    def carried(passed, factor, value, reverse):
        factor = jnp.where(passed, factor, 1.0)
        value = jnp.where(passed, value, 0.0)
        if reverse:
            factor, value = factor[::-1], value[::-1]
        return joined_by_halves((factor, value), compose)[1]

    inflow_later = carried(at > here, maps[:, 0], maps[:, 1], True)
    inflow_earlier = carried(at < here, maps[:, 2], maps[:, 3], False)
    adjoint = jnp.stack(
        [
            later_local + later_prod * inflow_later[None, :],
            earlier_local + earlier_prod * inflow_earlier[None, :],
        ]
    )
    decay_grad = adjoint * (decay_factors * prior_state - drive_term * squared / norm_factor)
    drive_grad = adjoint * norm_factor
    rate_pre = (decay_grad * (-RATE_SCALE * decay_rate) * rate_gate * (1.0 - rate_gate)).astype(
        jnp.bfloat16
    )
    input_pre = (drive_grad * conv_full * input_gate * (1.0 - input_gate)).astype(jnp.bfloat16)
    conv_grad = drive_grad * input_gate
    conv_grad = conv_grad + jnp.einsum(
        "sthd,shcd->sthc",
        rate_pre.reshape(2, tok_rows, heads_local, head_width),
        rate_gate_w,
        preferred_element_type=jnp.float32,
    ).reshape(2, tok_rows, channels)
    conv_grad = conv_grad + jnp.einsum(
        "sthd,shcd->sthc",
        input_pre.reshape(2, tok_rows, heads_local, head_width),
        input_gate_w,
        preferred_element_type=jnp.float32,
    ).reshape(2, tok_rows, channels)
    reach = conv_taps.shape[1] - 1
    ring_on = [(i, i + 1) for i in range(shards - 1)]
    ring_back = [(target, source) for source, target in ring_on]
    edge = conv_grad.astype(jnp.bfloat16)
    after = lax.ppermute(edge[0, :reach], "sp", ring_back).astype(jnp.float32)
    before = lax.ppermute(edge[1, -reach:], "sp", ring_on).astype(jnp.float32)
    later_side = jnp.concatenate([conv_grad[0], after])
    earlier_side = jnp.concatenate([before, conv_grad[1]])
    taps_full = conv_taps.astype(jnp.float32)
    input_grad = jnp.zeros((tok_rows, channels), jnp.float32)
    for tap_index in range(reach + 1):
        upper = reach - tap_index
        input_grad = (
            input_grad
            + taps_full[0, tap_index] * later_side[upper : upper + tok_rows]
            + taps_full[1, tap_index] * earlier_side[tap_index : tap_index + tok_rows]
        )
    proj_grad_t = summed_on_arrival(
        jnp.einsum("td,tc->dc", mid_grad_b, mixed_b, preferred_element_type=jnp.float32).astype(
            jnp.bfloat16
        ),
        "sp",
        0,
    )
    return (
        gate_grad,
        up_grad,
        down_grad,
        proj_grad_t,
        input_grad.astype(jnp.bfloat16),
        branch_gate_grad,
    )


def solution(mesh):
    in_specs = (
        P("sp", None),
        P("sp", None),
        P("sp", None),
        P("sp", None),
        P("sp", None, "tp"),
        P("sp", None, "tp"),
        P("sp", "tp", None),
        P("tp", None),
        P("sp", "tp"),
        P(None, "sp", "tp"),
        P(None, "sp", "tp"),
        P(None, "tp", None, None),
        P(None, "tp", None, None),
        P(None, "tp"),
        P(None, "sp", "tp"),
        P(None, None, "tp"),
    )
    out_specs = (
        P("sp", None, "tp"),
        P("sp", None, "tp"),
        P("sp", "tp", None),
        P("sp", "tp"),
        P("sp", "tp"),
        P("sp", "tp"),
    )
    return jax.shard_map(
        on_device, mesh=mesh, in_specs=in_specs, out_specs=out_specs, check_vma=False
    )
```

```python
import jax
import jax.numpy as jnp
from jax import lax
from jax.experimental import pallas as pl
from jax.experimental.pallas import tpu as pltpu
from jax.sharding import PartitionSpec as P

RATE_SCALE = 8.0
CLAMP_LIMIT = 7.0
SHARPNESS = 1.702
NORM_EPSILON = 1e-06
STATE_FLOOR = 0.001
GELU_CUBIC = 0.044715
GELU_SCALE = 0.7978845608028654
LANES = 128


def in_blocks(x, dim, count):
    dims = x.shape
    tiles = x.reshape(*dims[:dim], count, dims[dim] // count, *dims[dim + 1 :])
    return jnp.moveaxis(tiles, dim, 0)


def summed_on_arrival(x, axis, dim):
    tiles = in_blocks(x, dim, lax.axis_size(axis))
    arrived = lax.all_to_all(tiles, axis, split_axis=0, concat_axis=0, tiled=True)
    return arrived.astype(jnp.float32).sum(axis=0)


def ring_pairs(axis):
    count = lax.axis_size(axis)
    forward = [(i, (i + 1) % count) for i in range(count)]
    return forward, [(target, source) for source, target in forward]


def ring_blocks(x, axis):
    forward, backward = ring_pairs(axis)
    half = x.shape[0] // 2
    left = lax.ppermute(x, axis, forward)
    right = lax.ppermute(x, axis, backward)
    far_top = lax.ppermute(left[:half], axis, forward)
    far_bottom = lax.ppermute(right[half:], axis, backward)
    return x, right, jnp.concatenate([far_top, far_bottom], axis=0), left


def ring_sum(partial, half, axis):
    forward, backward = ring_pairs(axis)
    far = partial(2).astype(jnp.bfloat16)
    from_left = lax.ppermute(far[:half], axis, forward).astype(jnp.float32)
    from_right = lax.ppermute(far[half:], axis, backward).astype(jnp.float32)
    to_right, to_left = partial(1), partial(3)
    to_right = jnp.concatenate([to_right[:half] + from_left, to_right[half:]])
    to_left = jnp.concatenate([to_left[:half], to_left[half:] + from_right])
    got_left = lax.ppermute(to_right.astype(jnp.bfloat16), axis, forward)
    got_right = lax.ppermute(to_left.astype(jnp.bfloat16), axis, backward)
    return partial(0) + got_left.astype(jnp.float32) + got_right.astype(jnp.float32)


def laid_out(tiles, dim):
    tiles = jnp.moveaxis(tiles, 0, dim)
    dims = tiles.shape
    return tiles.reshape(*dims[:dim], dims[dim] * dims[dim + 1], *dims[dim + 2 :])


def sent_to_all(x, axis):
    copies = jnp.broadcast_to(x, (lax.axis_size(axis), *x.shape))
    return lax.all_to_all(copies, axis, split_axis=0, concat_axis=0, tiled=True)


def gathered_copies(x, axis, dim):
    return laid_out(sent_to_all(x, axis), dim)


def gelu_parts(values):
    inside = GELU_SCALE * (values + GELU_CUBIC * values * values * values)
    tangent = jnp.tanh(inside)
    result = 0.5 * values * (1.0 + tangent)
    slope_value = 0.5 * (1.0 + tangent) + 0.5 * values * (1.0 - tangent * tangent) * GELU_SCALE * (
        1.0 + 3.0 * GELU_CUBIC * values * values
    )
    return (result, slope_value)


SEGMENTS = 8
EDGE = 8


def over_segments(a_rows, b_rows, order):
    carry, factor = jnp.zeros_like(a_rows[:1]), jnp.ones_like(a_rows[:1])
    carries, factors = [None] * SEGMENTS, [None] * SEGMENTS
    for s in order:
        carries[s], factors[s] = carry, factor
        a, b = a_rows[s : s + 1], b_rows[s : s + 1]
        carry, factor = a * carry + b, a * factor
    return jnp.concatenate(carries), jnp.concatenate(factors), factor, carry


def scan_side(seed_ref, decay_ref, local_ref, prod_ref, base, rows, reverse):
    step = rows // SEGMENTS

    def at(i):
        return pl.ds(base + i, SEGMENTS, stride=step)

    order = list(range(step))[::-1] if reverse else list(range(step))
    value = factor = last = None
    for i in order:
        seed = seed_ref[pl.ds(i, SEGMENTS, stride=step), :]
        value = seed if value is None else seed + last * value
        factor = jnp.ones_like(seed) if factor is None else factor * last
        local_ref[at(i), :] = value
        prod_ref[at(i), :] = factor
        last = decay_ref[at(i), :]
    segs = range(SEGMENTS)[::-1] if reverse else range(SEGMENTS)
    carries, factors, whole_factor, whole_value = over_segments(
        factor * last, value * last, segs
    )
    for i in range(step):
        prod = prod_ref[at(i), :]
        local_ref[at(i), :] = local_ref[at(i), :] + prod * carries
        prod_ref[at(i), :] = prod * factors
    return whole_factor, whole_value


def branch_kernel(
    token_ref,
    mid_ref,
    inv_ref,
    cot_ref,
    out_proj_ref,
    states_ref,
    gelu_ref,
    slope_ref,
    decay_ref,
    first_ref,
    last_ref,
    mid_grad_ref,
    gate_out_ref,
    local_ref,
    prod_ref,
    map_ref,
    low_ref,
    high_ref,
    seed_ref,
):
    groups, rows, span = token_ref.shape
    inv = inv_ref[...]
    total = jnp.zeros_like(inv)
    for k in range(groups):
        cols = slice(k * span, (k + 1) * span)
        normed = mid_ref[:, cols].astype(jnp.float32) * inv
        total = total + jnp.sum(
            token_ref[k].astype(jnp.float32) * normed, axis=1, keepdims=True
        )
    mean = total / (groups * span)
    branch = jnp.zeros(states_ref.shape, jnp.float32)
    for k in range(groups):
        cols = slice(k * span, (k + 1) * span)
        normed = mid_ref[:, cols].astype(jnp.float32) * inv
        grad = (
            cot_ref[:, cols].astype(jnp.float32)
            + inv * (token_ref[k].astype(jnp.float32) - normed * mean)
        ).astype(jnp.bfloat16)
        mid_grad_ref[:, cols] = grad
        branch = branch + lax.dot_general(
            grad,
            out_proj_ref[:, cols],
            (((1,), (1,)), ((), ())),
            preferred_element_type=jnp.float32,
        )
    gate_out_ref[...] = (branch * states_ref[...] * slope_ref[...]).astype(jnp.bfloat16)
    seed_ref[...] = branch * gelu_ref[...]
    later = scan_side(seed_ref, decay_ref, local_ref, prod_ref, 0, rows, True)
    earlier = scan_side(seed_ref, decay_ref, local_ref, prod_ref, rows, rows, False)
    map_ref[...] = jnp.concatenate([*later, *earlier])
    low_ref[:EDGE] = local_ref[:EDGE]
    low_ref[EDGE : 2 * EDGE] = prod_ref[:EDGE]
    low_ref[2 * EDGE :] = first_ref[...]
    high_ref[:EDGE] = local_ref[2 * rows - EDGE :]
    high_ref[EDGE : 2 * EDGE] = prod_ref[2 * rows - EDGE :]
    high_ref[2 * EDGE :] = last_ref[...]


def folded(maps_ref, which, kept, reverse):
    count = maps_ref.shape[0] // 4
    step = count // SEGMENTS
    lead = step * lax.broadcasted_iota(jnp.int32, (SEGMENTS, LANES), 0)
    value = jnp.zeros((SEGMENTS, LANES), jnp.float32)
    factor = jnp.ones((SEGMENTS, LANES), jnp.float32)
    for i in range(step)[::-1] if reverse else range(step):
        use = kept(lead + i)
        a = maps_ref[pl.ds(4 * i + which, SEGMENTS, stride=4 * step), :]
        b = maps_ref[pl.ds(4 * i + which + 1, SEGMENTS, stride=4 * step), :]
        a, b = jnp.where(use, a, 1.0), jnp.where(use, b, 0.0)
        value, factor = a * value + b, factor * a
    carry = jnp.zeros((1, LANES), jnp.float32)
    for s in range(SEGMENTS)[::-1] if reverse else range(SEGMENTS):
        carry = factor[s : s + 1] * carry + value[s : s + 1]
    return carry


def tail_kernel(
    here_ref,
    maps_ref,
    local_ref,
    prod_ref,
    drive_ref,
    rate_ref,
    input_ref,
    after_ref,
    before_ref,
    rate_w_ref,
    input_w_ref,
    taps_ref,
    out_ref,
    later_ref,
    earlier_ref,
):
    here = here_ref[0]
    rows = out_ref.shape[0]
    reach = taps_ref.shape[0] // 2 - 1

    def spread(side, adjoint, drive, rate, inp):
        def back(coef, w_ref):
            return lax.dot_general(
                (adjoint * coef).astype(jnp.bfloat16),
                w_ref[side],
                (((1,), (1,)), ((), ())),
                preferred_element_type=jnp.float32,
            )

        return adjoint * drive + back(rate, rate_w_ref) + back(inp, input_w_ref)

    def main(side, inflow):
        own = slice(side * rows, (side + 1) * rows)
        adjoint = local_ref[own] + prod_ref[own] * inflow
        return spread(side, adjoint, drive_ref[own], rate_ref[own], input_ref[own])

    def edge(side, ref, inflow):
        part = [ref[k * EDGE : (k + 1) * EDGE] for k in range(5)]
        return spread(side, part[0] + part[1] * inflow, *part[2:])

    later_ref[:rows] = main(0, folded(maps_ref, 0, lambda j: j > here, True))
    later_ref[rows:] = edge(0, after_ref, folded(maps_ref, 0, lambda j: j > here + 1, True))
    earlier_ref[:EDGE] = edge(
        1, before_ref, folded(maps_ref, 2, lambda j: j < here - 1, False)
    )
    earlier_ref[EDGE:] = main(1, folded(maps_ref, 2, lambda j: j < here, False))
    total = jnp.zeros((rows, LANES), jnp.float32)
    for k in range(reach + 1):
        up, down = reach - k, EDGE - reach + k
        total = total + taps_ref[k : k + 1] * later_ref[up : up + rows]
        total = (
            total
            + taps_ref[reach + 1 + k : reach + 2 + k] * earlier_ref[down : down + rows]
        )
    out_ref[...] = total.astype(jnp.bfloat16)


def on_device(
    mid,
    out_grad,
    expert_ids,
    route_weights,
    gate_proj,
    up_proj,
    down_proj,
    out_proj,
    branch_gate,
    conv_out,
    prior_state,
    rate_gate_w,
    input_gate_w,
    decay_param,
    decay_jump,
    conv_taps,
):
    tok_rows, embedding_width = mid.shape
    shards = lax.axis_size("sp")
    groups = lax.axis_size("tp")
    local_experts = gate_proj.shape[0]
    experts_all = local_experts * shards
    top_count = expert_ids.shape[1]
    expert_room = 3 * top_count * tok_rows // (2 * experts_all)
    slot_count = experts_all * expert_room
    mid_full = mid.astype(jnp.float32)
    inv_rms = lax.rsqrt(jnp.mean(mid_full * mid_full, axis=1, keepdims=True) + NORM_EPSILON)
    normed = mid_full * inv_rms
    normed_b = normed.astype(jnp.bfloat16)
    flat_ids = expert_ids.reshape(-1)
    onehot = (flat_ids[:, None] == jnp.arange(experts_all, dtype=jnp.int32)[None, :]).astype(
        jnp.int32
    )
    rank_ids = jnp.sum((jnp.cumsum(onehot, axis=0) - onehot) * onehot, axis=1)
    slot_ids = (flat_ids * expert_room + rank_ids).reshape(tok_rows, top_count)
    matches = slot_ids[None, :, :] == jnp.arange(slot_count, dtype=jnp.int32)[:, None, None]
    select = jnp.any(matches, axis=2).astype(jnp.bfloat16)
    slot_gate = jnp.sum(jnp.where(matches, route_weights[None, :, :], 0.0), axis=(1, 2))
    heads_local = rate_gate_w.shape[1]
    head_width = rate_gate_w.shape[2]
    channels = heads_local * head_width

    def on_diagonal(w):
        return jnp.concatenate(
            [
                jnp.pad(
                    w[:, h],
                    ((0, 0), (0, 0), (h * head_width, channels - (h + 1) * head_width)),
                )
                for h in range(heads_local)
            ],
            axis=1,
        )

    rate_blocks, input_blocks = on_diagonal(rate_gate_w), on_diagonal(input_gate_w)

    def gate_of(blocks):
        return jax.nn.sigmoid(
            jnp.einsum("stc,scd->std", conv_out, blocks, preferred_element_type=jnp.float32)
        )

    rate_gate, input_gate = gate_of(rate_blocks), gate_of(input_blocks)
    decay_rate = jax.nn.softplus(-decay_param)[:, None, :]
    log_decay = -RATE_SCALE * rate_gate * decay_rate + decay_jump
    decay_factors = jnp.exp(log_decay)
    squared = jnp.exp(2.0 * log_decay)
    norm_factor = jnp.sqrt(STATE_FLOOR - jnp.expm1(2.0 * log_decay))
    conv_full = conv_out.astype(jnp.float32)
    drive_term = input_gate * conv_full
    decayed = decay_factors * prior_state
    states = decayed + norm_factor * drive_term
    summed_states = states[0] + states[1]
    gelu_value, gelu_slope = gelu_parts(branch_gate.astype(jnp.float32))
    mixed_b = (summed_states * gelu_value).astype(jnp.bfloat16)
    rate_coef = (
        (decayed - drive_term * squared / norm_factor)
        * (-RATE_SCALE * decay_rate)
        * rate_gate
        * (1.0 - rate_gate)
    )
    drive_coef = norm_factor * input_gate
    input_coef = norm_factor * conv_full * input_gate * (1.0 - input_gate)
    first_edge = jnp.concatenate([c[0, :EDGE] for c in (drive_coef, rate_coef, input_coef)])
    last_edge = jnp.concatenate([c[1, -EDGE:] for c in (drive_coef, rate_coef, input_coef)])
    place = lax.axis_index("tp")
    span = embedding_width // groups

    def packed(x):
        return x.reshape(shards, -1, LANES)

    def turned(x, dim):
        return jnp.concatenate(
            [
                lax.dynamic_slice_in_dim(x, ((place + k) % groups) * span, span, dim)
                for k in range(groups)
            ],
            axis=dim,
        )

    rows_source = lax.dynamic_slice_in_dim(normed_b, place * span, span, 1)
    grad_source = lax.dynamic_slice_in_dim(out_grad, place * span, span, 1)
    sent_rows = jnp.dot(select, rows_source, preferred_element_type=jnp.float32).astype(
        jnp.bfloat16
    )
    sent_grad = (
        jnp.dot(select, grad_source, preferred_element_type=jnp.float32) * slot_gate[:, None]
    ).astype(jnp.bfloat16)
    got_rows = lax.all_to_all(packed(sent_rows), "sp", 0, 0, tiled=True).reshape(slot_count, span)
    got_grad = lax.all_to_all(packed(sent_grad), "sp", 0, 0, tiled=True).reshape(slot_count, span)
    rows = ring_blocks(got_rows, "tp")
    grads = ring_blocks(got_grad, "tp")
    both_proj = jnp.concatenate([turned(gate_proj[0], 0), turned(up_proj[0], 0)], axis=1)
    down_turned = turned(down_proj[0], 1)
    hidden = gate_proj.shape[2]
    pre = sum(
        jnp.dot(
            rows[k], both_proj[k * span : (k + 1) * span], preferred_element_type=jnp.float32
        )
        for k in range(groups)
    )
    gate_pre, up_pre = pre[:, :hidden], pre[:, hidden:]
    gate_clamped = jnp.minimum(gate_pre, CLAMP_LIMIT)
    up_clamped = jnp.clip(up_pre, -CLAMP_LIMIT, CLAMP_LIMIT)
    gate_sigmoid = jax.nn.sigmoid(SHARPNESS * gate_clamped)
    swish_value = gate_clamped * gate_sigmoid
    act_b = ((up_clamped + 1.0) * swish_value).astype(jnp.bfloat16)
    act_grad = sum(
        jnp.einsum(
            "rd,fd->rf",
            grads[k],
            down_turned[:, k * span : (k + 1) * span],
            preferred_element_type=jnp.float32,
        )
        for k in range(groups)
    )
    gate_delta = jnp.where(
        gate_pre < CLAMP_LIMIT,
        act_grad
        * (up_clamped + 1.0)
        * (gate_sigmoid + SHARPNESS * swish_value * (1.0 - gate_sigmoid)),
        0.0,
    ).astype(jnp.bfloat16)
    up_delta = jnp.where(jnp.abs(up_pre) < CLAMP_LIMIT, act_grad * swish_value, 0.0).astype(
        jnp.bfloat16
    )
    deltas = jnp.concatenate([gate_delta, up_delta], axis=1)

    def partial(k):
        return jnp.einsum(
            "rf,df->rd",
            deltas,
            both_proj[k * span : (k + 1) * span],
            preferred_element_type=jnp.float32,
        )

    summed = ring_sum(partial, slot_count // 2, "tp")
    returned = lax.all_to_all(packed(summed.astype(jnp.bfloat16)), "sp", 0, 0, tiled=True).reshape(
        slot_count, span
    )

    def in_order(blocks):
        stack = jnp.stack(blocks)
        return jnp.concatenate(
            [
                lax.dynamic_index_in_dim(stack, (k - place) % groups, 0, keepdims=False)
                for k in range(groups)
            ],
            axis=1,
        )

    expert_rows, expert_grads, deltas_late, act_late = lax.optimization_barrier(
        (in_order(rows), in_order(grads), deltas, act_b)
    )
    down_grad = jnp.einsum(
        "rf,rd->fd", act_late, expert_grads, preferred_element_type=jnp.float32
    ).astype(jnp.bfloat16)[None]
    gate_grad = jnp.einsum(
        "rd,rf->df", expert_rows, deltas_late[:, :hidden], preferred_element_type=jnp.float32
    ).astype(jnp.bfloat16)[None]
    up_grad = jnp.einsum(
        "rd,rf->df", expert_rows, deltas_late[:, hidden:], preferred_element_type=jnp.float32
    ).astype(jnp.bfloat16)[None]
    token_part = jnp.einsum("st,sd->td", select, returned, preferred_element_type=jnp.float32)
    token_grad = sent_to_all(token_part.astype(jnp.bfloat16), "tp")
    f32 = jnp.float32
    wide = jax.ShapeDtypeStruct((2 * tok_rows, channels), f32)
    edges = jax.ShapeDtypeStruct((5 * EDGE, channels), f32)
    mid_grad_b, branch_gate_grad, local, prod, maps, low, high = pl.pallas_call(
        branch_kernel,
        out_shape=(
            jax.ShapeDtypeStruct((tok_rows, embedding_width), jnp.bfloat16),
            jax.ShapeDtypeStruct((tok_rows, channels), jnp.bfloat16),
            wide,
            wide,
            jax.ShapeDtypeStruct((4, channels), f32),
            edges,
            edges,
        ),
        scratch_shapes=[pltpu.VMEM((tok_rows, channels), f32)],
        name="branch",
    )(
        token_grad,
        mid,
        inv_rms,
        out_grad,
        out_proj,
        summed_states,
        gelu_value,
        gelu_slope,
        decay_factors.reshape(2 * tok_rows, channels),
        first_edge,
        last_edge,
    )
    ring_on = [(i, i + 1) for i in range(shards - 1)]
    ring_back = [(target, source) for source, target in ring_on]
    all_maps = sent_to_all(maps, "sp").reshape(4 * shards, channels)
    after = lax.ppermute(low, "sp", ring_back)
    before = lax.ppermute(high, "sp", ring_on)
    here = lax.axis_index("sp").astype(jnp.int32).reshape(1)
    vmem = pl.BlockSpec(memory_space=pltpu.VMEM)
    input_grad = pl.pallas_call(
        tail_kernel,
        out_shape=jax.ShapeDtypeStruct((tok_rows, channels), jnp.bfloat16),
        in_specs=[pl.BlockSpec(memory_space=pltpu.SMEM)] + [vmem] * 11,
        scratch_shapes=[pltpu.VMEM((tok_rows + EDGE, channels), f32)] * 2,
        name="tail",
    )(
        here,
        all_maps,
        local,
        prod,
        drive_coef.reshape(2 * tok_rows, channels),
        rate_coef.reshape(2 * tok_rows, channels),
        input_coef.reshape(2 * tok_rows, channels),
        after,
        before,
        rate_blocks,
        input_blocks,
        conv_taps.astype(f32).reshape(-1, channels),
    )
    proj_grad_t = summed_on_arrival(
        jnp.einsum("td,tc->dc", mid_grad_b, mixed_b, preferred_element_type=f32).astype(
            jnp.bfloat16
        ),
        "sp",
        0,
    )
    return (gate_grad, up_grad, down_grad, proj_grad_t, input_grad, branch_gate_grad)


def solution(mesh):
    in_specs = (
        P("sp", None),
        P("sp", None),
        P("sp", None),
        P("sp", None),
        P("sp", None, "tp"),
        P("sp", None, "tp"),
        P("sp", "tp", None),
        P("tp", None),
        P("sp", "tp"),
        P(None, "sp", "tp"),
        P(None, "sp", "tp"),
        P(None, "tp", None, None),
        P(None, "tp", None, None),
        P(None, "tp"),
        P(None, "sp", "tp"),
        P(None, None, "tp"),
    )
    out_specs = (
        P("sp", None, "tp"),
        P("sp", None, "tp"),
        P("sp", "tp", None),
        P("sp", "tp"),
        P("sp", "tp"),
        P("sp", "tp"),
    )
    return jax.shard_map(
        on_device, mesh=mesh, in_specs=in_specs, out_specs=out_specs, check_vma=False
    )
```

```python
import jax
import jax.numpy as jnp
from jax import lax
from jax.experimental import pallas as pl
from jax.experimental.pallas import tpu as pltpu
from jax.sharding import PartitionSpec as P

RATE_SCALE = 8.0
CLAMP_LIMIT = 7.0
SHARPNESS = 1.702
NORM_EPSILON = 1e-06
STATE_FLOOR = 0.001
GELU_CUBIC = 0.044715
GELU_SCALE = 0.7978845608028654
LANES = 128


def ring_pairs(axis):
    count = lax.axis_size(axis)
    forward = [(i, (i + 1) % count) for i in range(count)]
    return forward, [(target, source) for source, target in forward]


def ring_blocks(x, axis):
    forward, backward = ring_pairs(axis)
    half = x.shape[0] // 2
    left = lax.ppermute(x, axis, forward)
    right = lax.ppermute(x, axis, backward)
    far_top = lax.ppermute(left[:half], axis, forward)
    far_bottom = lax.ppermute(right[half:], axis, backward)
    return x, right, far_top, far_bottom, left


def sent_to_all(x, axis):
    copies = jnp.broadcast_to(x, (lax.axis_size(axis), *x.shape))
    return lax.all_to_all(copies, axis, split_axis=0, concat_axis=0, tiled=True)


def gelu_parts(values):
    inside = GELU_SCALE * (values + GELU_CUBIC * values * values * values)
    tangent = jnp.tanh(inside)
    result = 0.5 * values * (1.0 + tangent)
    slope_value = 0.5 * (1.0 + tangent) + 0.5 * values * (1.0 - tangent * tangent) * GELU_SCALE * (
        1.0 + 3.0 * GELU_CUBIC * values * values
    )
    return (result, slope_value)


SEGMENTS = 8
EDGE = 8


def over_segments(a_rows, b_rows, order):
    carry, factor = jnp.zeros_like(a_rows[:1]), jnp.ones_like(a_rows[:1])
    carries, factors = [None] * SEGMENTS, [None] * SEGMENTS
    for s in order:
        carries[s], factors[s] = carry, factor
        a, b = a_rows[s : s + 1], b_rows[s : s + 1]
        carry, factor = a * carry + b, a * factor
    return jnp.concatenate(carries), jnp.concatenate(factors), factor, carry


def scan_side(seed_ref, decay_ref, local_ref, prod_ref, base, rows, reverse):
    step = rows // SEGMENTS

    def at(i):
        return pl.ds(base + i, SEGMENTS, stride=step)

    order = list(range(step))[::-1] if reverse else list(range(step))
    value = factor = last = None
    for i in order:
        seed = seed_ref[pl.ds(i, SEGMENTS, stride=step), :]
        value = seed if value is None else seed + last * value
        factor = jnp.ones_like(seed) if factor is None else factor * last
        local_ref[at(i), :] = value
        prod_ref[at(i), :] = factor
        last = decay_ref[at(i), :]
    segs = range(SEGMENTS)[::-1] if reverse else range(SEGMENTS)
    carries, factors, whole_factor, whole_value = over_segments(
        factor * last, value * last, segs
    )
    for i in range(step):
        prod = prod_ref[at(i), :]
        local_ref[at(i), :] = local_ref[at(i), :] + prod * carries
        prod_ref[at(i), :] = prod * factors
    return whole_factor, whole_value


def branch_kernel(
    token_ref,
    mid_ref,
    inv_ref,
    cot_ref,
    out_proj_ref,
    states_ref,
    gelu_ref,
    slope_ref,
    decay_ref,
    mixed_ref,
    first_ref,
    last_ref,
    gate_out_ref,
    local_ref,
    prod_ref,
    send_ref,
    low_ref,
    high_ref,
    seed_ref,
):
    shards = send_ref.shape[0]
    share = shards // token_ref.shape[0]
    piece = token_ref.shape[2] // share
    groups, rows, span = token_ref.shape
    inv = inv_ref[...]
    total = jnp.zeros_like(inv)
    for k in range(groups):
        cols = slice(k * span, (k + 1) * span)
        normed = mid_ref[:, cols].astype(jnp.float32) * inv
        total = total + jnp.sum(
            token_ref[k].astype(jnp.float32) * normed, axis=1, keepdims=True
        )
    mean = total / (groups * span)
    branch = jnp.zeros(states_ref.shape, jnp.float32)
    for k in range(groups):
        cols = slice(k * span, (k + 1) * span)
        normed = mid_ref[:, cols].astype(jnp.float32) * inv
        grad = (
            cot_ref[:, cols].astype(jnp.float32)
            + inv * (token_ref[k].astype(jnp.float32) - normed * mean)
        ).astype(jnp.bfloat16)
        branch = branch + last_dims(grad, out_proj_ref[:, cols])
        proj = first_dims(grad, mixed_ref[...]).astype(jnp.bfloat16)
        send_ref[k * share : (k + 1) * share, :piece, :] = proj.reshape(share, piece, LANES)
    gate_out_ref[...] = (branch * states_ref[...] * slope_ref[...]).astype(jnp.bfloat16)
    seed_ref[...] = branch * gelu_ref[...]
    later = scan_side(seed_ref, decay_ref, local_ref, prod_ref, 0, rows, True)
    earlier = scan_side(seed_ref, decay_ref, local_ref, prod_ref, rows, rows, False)
    maps = jnp.concatenate([*later, *earlier])
    high_part = maps.astype(jnp.bfloat16)
    low_part = (maps - high_part.astype(jnp.float32)).astype(jnp.bfloat16)
    pair = jnp.concatenate(
        [high_part.astype(jnp.float32), low_part.astype(jnp.float32)]
    ).astype(jnp.bfloat16)
    send_ref[:, piece:, :] = jnp.broadcast_to(pair[None], (shards, *pair.shape))
    low_ref[:EDGE] = local_ref[:EDGE]
    low_ref[EDGE : 2 * EDGE] = prod_ref[:EDGE]
    low_ref[2 * EDGE :] = first_ref[...]
    high_ref[:EDGE] = local_ref[2 * rows - EDGE :]
    high_ref[EDGE : 2 * EDGE] = prod_ref[2 * rows - EDGE :]
    high_ref[2 * EDGE :] = last_ref[...]


def folded(maps_ref, which, kept, reverse):
    count = maps_ref.shape[0] // 8
    step = count // SEGMENTS
    lead = step * lax.broadcasted_iota(jnp.int32, (SEGMENTS, LANES), 0)
    value = jnp.zeros((SEGMENTS, LANES), jnp.float32)
    factor = jnp.ones((SEGMENTS, LANES), jnp.float32)
    for i in range(step)[::-1] if reverse else range(step):
        use = kept(lead + i)
        a, b = (
            maps_ref[pl.ds(8 * i + q, SEGMENTS, stride=8 * step), :]
            + maps_ref[pl.ds(8 * i + q + 4, SEGMENTS, stride=8 * step), :]
            for q in (which, which + 1)
        )
        a, b = jnp.where(use, a, 1.0), jnp.where(use, b, 0.0)
        value, factor = a * value + b, factor * a
    carry = jnp.zeros((1, LANES), jnp.float32)
    for s in range(SEGMENTS)[::-1] if reverse else range(SEGMENTS):
        carry = factor[s : s + 1] * carry + value[s : s + 1]
    return carry


def tail_kernel(
    here_ref,
    got_ref,
    local_ref,
    prod_ref,
    drive_ref,
    rate_ref,
    input_ref,
    after_ref,
    before_ref,
    rate_w_ref,
    input_w_ref,
    taps_ref,
    out_ref,
    proj_ref,
    later_ref,
    earlier_ref,
    maps_ref,
):
    here = here_ref[0]
    piece = proj_ref.shape[0]
    proj_ref[...] = jnp.sum(got_ref[:, :piece, :].astype(jnp.float32), axis=0)
    maps_ref[...] = got_ref[:, piece:, :].astype(jnp.float32).reshape(maps_ref.shape)
    rows = out_ref.shape[0]
    reach = taps_ref.shape[0] // 2 - 1

    def spread(side, adjoint, drive, rate, inp):
        def back(coef, w_ref):
            return lax.dot_general(
                (adjoint * coef).astype(jnp.bfloat16),
                w_ref[side],
                (((1,), (1,)), ((), ())),
                preferred_element_type=jnp.float32,
            )

        return adjoint * drive + back(rate, rate_w_ref) + back(inp, input_w_ref)

    def main(side, inflow):
        own = slice(side * rows, (side + 1) * rows)
        adjoint = local_ref[own] + prod_ref[own] * inflow
        return spread(side, adjoint, drive_ref[own], rate_ref[own], input_ref[own])

    def edge(side, ref, inflow):
        part = [ref[k * EDGE : (k + 1) * EDGE] for k in range(5)]
        return spread(side, part[0] + part[1] * inflow, *part[2:])

    later_ref[:rows] = main(0, folded(maps_ref, 0, lambda j: j > here, True))
    later_ref[rows:] = edge(0, after_ref, folded(maps_ref, 0, lambda j: j > here + 1, True))
    earlier_ref[:EDGE] = edge(
        1, before_ref, folded(maps_ref, 2, lambda j: j < here - 1, False)
    )
    earlier_ref[EDGE:] = main(1, folded(maps_ref, 2, lambda j: j < here, False))
    total = jnp.zeros((rows, LANES), jnp.float32)
    for k in range(reach + 1):
        up, down = reach - k, EDGE - reach + k
        total = total + taps_ref[k : k + 1] * later_ref[up : up + rows]
        total = (
            total
            + taps_ref[reach + 1 + k : reach + 2 + k] * earlier_ref[down : down + rows]
        )
    out_ref[...] = total.astype(jnp.bfloat16)


ROOM_PAD = 40


def row_of(slot, part, parts):
    return slot * parts + part


def pack_rows(value, scratch_ref, out_ref, room):
    shards = out_ref.shape[0]
    parts = value.shape[1] // LANES
    for r in range(room):
        for c in range(parts):
            scratch_ref[pl.ds(row_of(r, c, parts), shards, stride=ROOM_PAD), :] = value[
                r * shards : (r + 1) * shards, c * LANES : (c + 1) * LANES
            ]
    for extra in range(room * parts, ROOM_PAD):
        scratch_ref[pl.ds(extra, shards, stride=ROOM_PAD), :] = jnp.zeros(
            (shards, LANES), jnp.float32
        )
    out_ref[...] = scratch_ref[...].reshape(out_ref.shape).astype(jnp.bfloat16)


def unpack_rows(in_ref, scratch_ref, out_ref, room):
    shards = in_ref.shape[0]
    parts = out_ref.shape[1] // LANES
    scratch_ref[...] = in_ref[...].astype(jnp.float32).reshape(scratch_ref.shape)
    for r in range(room):
        for c in range(parts):
            out_ref[r * shards : (r + 1) * shards, c * LANES : (c + 1) * LANES] = scratch_ref[
                pl.ds(row_of(r, c, parts), shards, stride=ROOM_PAD), :
            ].astype(jnp.bfloat16)


def first_dims(a, b):
    return lax.dot_general(a, b, (((0,), (0,)), ((), ())), preferred_element_type=jnp.float32)


def last_dims(a, b):
    return lax.dot_general(a, b, (((1,), (1,)), ((), ())), preferred_element_type=jnp.float32)


def plain(a, b):
    return jnp.dot(a, b, preferred_element_type=jnp.float32)


def route_kernel(
    place_ref, ids_ref, mid_ref, packed_ref, inv_ref, pick0_ref, pick1_ref, scratch_ref
):
    rows, width = mid_ref.shape
    shards = packed_ref.shape[0]
    slots = pick0_ref.shape[1]
    span = packed_ref.shape[1] * LANES // (slots // shards) // LANES * LANES
    ids = ids_ref[...]
    lanes = lax.broadcasted_iota(jnp.int32, (rows, LANES), 1)
    hits = [ids[:, k : k + 1] == lanes for k in range(2)]
    named = (hits[0] | hits[1]).astype(jnp.bfloat16)
    above = (
        lax.broadcasted_iota(jnp.int32, (rows, rows), 0)
        > lax.broadcasted_iota(jnp.int32, (rows, rows), 1)
    ).astype(jnp.bfloat16)
    ranks = plain(above, named)
    wide = lax.broadcasted_iota(jnp.int32, (rows, slots), 1)
    picks = []
    for k, ref in enumerate((pick0_ref, pick1_ref)):
        rank = jnp.sum(jnp.where(hits[k], ranks, 0.0), axis=1, keepdims=True)
        target = rank.astype(jnp.int32) * shards + ids[:, k : k + 1]
        pick = (wide == target).astype(jnp.bfloat16)
        ref[...] = pick
        picks.append(pick)
    total = jnp.zeros((rows, 1), jnp.float32)
    step = 512
    for c in range(width // step):
        part = mid_ref[:, c * step : (c + 1) * step].astype(jnp.float32)
        total = total + jnp.sum(part * part, axis=1, keepdims=True)
    inv = lax.rsqrt(total / width + NORM_EPSILON)
    inv_ref[...] = inv
    own = mid_ref[:, pl.ds(pl.multiple_of(place_ref[0] * span, LANES), span)]
    normed = (own.astype(jnp.float32) * inv).astype(jnp.bfloat16)
    pack_rows(
        first_dims(picks[0] + picks[1], normed), scratch_ref, packed_ref, slots // shards
    )


def weigh_kernel(place_ref, weights_ref, cot_ref, pick0_ref, pick1_ref, packed_ref, scratch_ref):
    shards = packed_ref.shape[0]
    slots = pick0_ref.shape[1]
    span = packed_ref.shape[1] * LANES // (slots // shards) // LANES * LANES
    own = cot_ref[:, pl.ds(pl.multiple_of(place_ref[0] * span, LANES), span)].astype(jnp.float32)
    total = jnp.zeros((slots, span), jnp.float32)
    for k, ref in enumerate((pick0_ref, pick1_ref)):
        weighed = (own * weights_ref[:, k : k + 1]).astype(jnp.bfloat16)
        total = total + first_dims(ref[...], weighed)
    pack_rows(total, scratch_ref, packed_ref, slots // shards)


def unpack_kernel(in_ref, out_ref, scratch_ref):
    unpack_rows(in_ref, scratch_ref, out_ref, out_ref.shape[0] // in_ref.shape[0])


def offsets(place_ref, groups, span):
    return [
        pl.multiple_of(lax.rem(place_ref[0] + k, groups) * span, span) for k in range(groups)
    ]


def forward_kernel(
    place_ref,
    own_ref,
    right_ref,
    top_ref,
    bottom_ref,
    left_ref,
    gate_ref,
    up_ref,
    act_ref,
    gate_factor_ref,
    up_factor_ref,
):
    half, span = top_ref.shape
    at = offsets(place_ref, gate_ref.shape[0] // span, span)
    far = jnp.concatenate([top_ref[...], bottom_ref[...]])

    def pre(w_ref):
        total = plain(own_ref[...], w_ref[pl.ds(at[0], span), :])
        total = total + plain(right_ref[...], w_ref[pl.ds(at[1], span), :])
        total = total + plain(left_ref[...], w_ref[pl.ds(at[3], span), :])
        return total + plain(far, w_ref[pl.ds(at[2], span), :])

    gate_pre = pre(gate_ref)
    up_pre = pre(up_ref)
    gate = jnp.minimum(gate_pre, CLAMP_LIMIT)
    up_one = jnp.clip(up_pre, -CLAMP_LIMIT, CLAMP_LIMIT) + 1.0
    sig = jax.nn.sigmoid(SHARPNESS * gate)
    swish = gate * sig
    act_ref[...] = (up_one * swish).astype(jnp.bfloat16)
    gate_factor_ref[...] = jnp.where(
        gate_pre < CLAMP_LIMIT, up_one * (sig + SHARPNESS * swish * (1.0 - sig)), 0.0
    )
    up_factor_ref[...] = jnp.where(jnp.abs(up_pre) < CLAMP_LIMIT, swish, 0.0)


def delta_kernel(
    place_ref,
    own_ref,
    right_ref,
    top_ref,
    bottom_ref,
    left_ref,
    down_ref,
    gate_ref,
    up_ref,
    gate_factor_ref,
    up_factor_ref,
    gate_delta_ref,
    up_delta_ref,
    far_ref,
):
    half, span = top_ref.shape
    at = offsets(place_ref, gate_ref.shape[0] // span, span)
    far = jnp.concatenate([top_ref[...], bottom_ref[...]])
    act_grad = last_dims(own_ref[...], down_ref[:, pl.ds(at[0], span)])
    act_grad = act_grad + last_dims(right_ref[...], down_ref[:, pl.ds(at[1], span)])
    act_grad = act_grad + last_dims(left_ref[...], down_ref[:, pl.ds(at[3], span)])
    act_grad = act_grad + last_dims(far, down_ref[:, pl.ds(at[2], span)])
    gate_delta = (act_grad * gate_factor_ref[...]).astype(jnp.bfloat16)
    up_delta = (act_grad * up_factor_ref[...]).astype(jnp.bfloat16)
    gate_delta_ref[...] = gate_delta
    up_delta_ref[...] = up_delta
    far_ref[...] = (
        last_dims(gate_delta, gate_ref[pl.ds(at[2], span), :])
        + last_dims(up_delta, up_ref[pl.ds(at[2], span), :])
    ).astype(jnp.bfloat16)


def partial_kernel(place_ref, gate_delta_ref, up_delta_ref, gate_ref, up_ref, *out_refs):
    span = out_refs[0].shape[1]
    at = offsets(place_ref, gate_ref.shape[0] // span, span)
    for k, ref in zip((1, 3, 0), out_refs):
        ref[...] = last_dims(gate_delta_ref[...], gate_ref[pl.ds(at[k], span), :]) + last_dims(
            up_delta_ref[...], up_ref[pl.ds(at[k], span), :]
        )


def relay_kernel(right_ref, left_ref, from_left_ref, from_right_ref, to_right_ref, to_left_ref):
    half = from_left_ref.shape[0]
    bf = jnp.bfloat16
    to_right_ref[:half] = (right_ref[:half] + from_left_ref[...].astype(jnp.float32)).astype(bf)
    to_right_ref[half:] = right_ref[half:].astype(bf)
    to_left_ref[:half] = left_ref[:half].astype(bf)
    to_left_ref[half:] = (left_ref[half:] + from_right_ref[...].astype(jnp.float32)).astype(bf)


def gather_kernel(own_ref, from_left_ref, from_right_ref, packed_ref, scratch_ref):
    total = (
        own_ref[...]
        + from_left_ref[...].astype(jnp.float32)
        + from_right_ref[...].astype(jnp.float32)
    )
    pack_rows(total, scratch_ref, packed_ref, total.shape[0] // packed_ref.shape[0])


def combine_kernel(in_ref, pick0_ref, pick1_ref, out_ref, scratch_ref, rows_ref):
    unpack_rows(in_ref, scratch_ref, rows_ref, rows_ref.shape[0] // in_ref.shape[0])
    out_ref[...] = plain(pick0_ref[...] + pick1_ref[...], rows_ref[...]).astype(jnp.bfloat16)


def weights_kernel(
    place_ref,
    r_own_ref,
    r_right_ref,
    r_top_ref,
    r_bottom_ref,
    r_left_ref,
    g_own_ref,
    g_right_ref,
    g_top_ref,
    g_bottom_ref,
    g_left_ref,
    act_ref,
    gate_delta_ref,
    up_delta_ref,
    gate_out_ref,
    up_out_ref,
    down_out_ref,
):
    half, span = r_top_ref.shape
    at = offsets(place_ref, gate_out_ref.shape[0] // span, span)
    rows = (r_own_ref, r_right_ref, (r_top_ref, r_bottom_ref), r_left_ref)
    grads = (g_own_ref, g_right_ref, (g_top_ref, g_bottom_ref), g_left_ref)
    bf = jnp.bfloat16

    def whole(block):
        if isinstance(block, tuple):
            return jnp.concatenate([part[...] for part in block])
        return block[...]

    for k in range(4):
        row = whole(rows[k])
        gate_out_ref[pl.ds(at[k], span), :] = first_dims(row, gate_delta_ref[...]).astype(bf)
        up_out_ref[pl.ds(at[k], span), :] = first_dims(row, up_delta_ref[...]).astype(bf)
        down_out_ref[:, pl.ds(at[k], span)] = first_dims(act_ref[...], whole(grads[k])).astype(bf)


def on_device(
    mid,
    out_grad,
    expert_ids,
    route_weights,
    gate_proj,
    up_proj,
    down_proj,
    out_proj,
    branch_gate,
    conv_out,
    prior_state,
    rate_gate_w,
    input_gate_w,
    decay_param,
    decay_jump,
    conv_taps,
):
    tok_rows, embedding_width = mid.shape
    shards = lax.axis_size("sp")
    groups = lax.axis_size("tp")
    local_experts = gate_proj.shape[0]
    experts_all = local_experts * shards
    top_count = expert_ids.shape[1]
    expert_room = 3 * top_count * tok_rows // (2 * experts_all)
    slot_count = experts_all * expert_room
    span = embedding_width // groups
    hidden = gate_proj.shape[2]
    bf16, f32 = (jnp.bfloat16, jnp.float32)

    def shaped(*dims, dtype=bf16):
        return jax.ShapeDtypeStruct(dims, dtype)

    vmem = pl.BlockSpec(memory_space=pltpu.VMEM)
    smem = pl.BlockSpec(memory_space=pltpu.SMEM)

    def kernel(body, outs, name, *args, scalar=None, scratch=(), flops=0):
        lead = () if scalar is None else (scalar,)
        return pl.pallas_call(
            body,
            out_shape=outs,
            in_specs=[smem] * len(lead) + [vmem] * len(args),
            scratch_shapes=list(scratch),
            name=name,
            cost_estimate=pl.CostEstimate(flops=flops, transcendentals=0, bytes_accessed=0),
        )(*lead, *args)

    packed_shape = shaped(shards, ROOM_PAD, LANES)
    pack_scratch = pltpu.VMEM((shards * ROOM_PAD, LANES), f32)
    place = lax.axis_index("tp").astype(jnp.int32).reshape(1)
    pick_shape = shaped(tok_rows, slot_count)
    sent_rows, inv_rms, pick0, pick1 = kernel(
        route_kernel,
        (packed_shape, shaped(tok_rows, 1, dtype=f32), pick_shape, pick_shape),
        "route",
        expert_ids,
        mid,
        scalar=place,
        scratch=(pack_scratch,),
    )
    sent_grad = kernel(
        weigh_kernel,
        packed_shape,
        "weigh",
        route_weights,
        out_grad,
        pick0,
        pick1,
        scalar=place,
        scratch=(pack_scratch,),
        flops=1 << 28,
    )
    heads_local = rate_gate_w.shape[1]
    head_width = rate_gate_w.shape[2]
    channels = heads_local * head_width

    def on_diagonal(w):
        return jnp.concatenate(
            [
                jnp.pad(
                    w[:, h],
                    ((0, 0), (0, 0), (h * head_width, channels - (h + 1) * head_width)),
                )
                for h in range(heads_local)
            ],
            axis=1,
        )

    rate_blocks, input_blocks = on_diagonal(rate_gate_w), on_diagonal(input_gate_w)

    def gate_of(blocks):
        return jax.nn.sigmoid(
            jnp.einsum("stc,scd->std", conv_out, blocks, preferred_element_type=jnp.float32)
        )

    rate_gate, input_gate = gate_of(rate_blocks), gate_of(input_blocks)
    decay_rate = jax.nn.softplus(-decay_param)[:, None, :]
    log_decay = -RATE_SCALE * rate_gate * decay_rate + decay_jump
    decay_factors = jnp.exp(log_decay)
    squared = jnp.exp(2.0 * log_decay)
    norm_factor = jnp.sqrt(STATE_FLOOR - jnp.expm1(2.0 * log_decay))
    conv_full = conv_out.astype(jnp.float32)
    drive_term = input_gate * conv_full
    decayed = decay_factors * prior_state
    states = decayed + norm_factor * drive_term
    summed_states = states[0] + states[1]
    gelu_value, gelu_slope = gelu_parts(branch_gate.astype(jnp.float32))
    mixed_b = (summed_states * gelu_value).astype(jnp.bfloat16)
    rate_coef = (
        (decayed - drive_term * squared / norm_factor)
        * (-RATE_SCALE * decay_rate)
        * rate_gate
        * (1.0 - rate_gate)
    )
    drive_coef = norm_factor * input_gate
    input_coef = norm_factor * conv_full * input_gate * (1.0 - input_gate)
    first_edge = jnp.concatenate([c[0, :EDGE] for c in (drive_coef, rate_coef, input_coef)])
    last_edge = jnp.concatenate([c[1, -EDGE:] for c in (drive_coef, rate_coef, input_coef)])
    (
        sent_grad,
        decay_factors,
        summed_states,
        gelu_value,
        gelu_slope,
        mixed_b,
        rate_coef,
        drive_coef,
        input_coef,
        first_edge,
        last_edge,
    ) = lax.optimization_barrier(
        (
            sent_grad,
            decay_factors,
            summed_states,
            gelu_value,
            gelu_slope,
            mixed_b,
            rate_coef,
            drive_coef,
            input_coef,
            first_edge,
            last_edge,
        )
    )

    def unpacked(x, name):
        return kernel(
            unpack_kernel, shaped(slot_count, span), name, x, scratch=(pack_scratch,)
        )

    got_rows = lax.all_to_all(sent_rows, "sp", 0, 0, tiled=True)
    rows = ring_blocks(unpacked(got_rows, "unpack_rows"), "tp")
    got_grad = lax.all_to_all(sent_grad, "sp", 0, 0, tiled=True)
    grads = ring_blocks(unpacked(got_grad, "unpack_grads"), "tp")
    wide_hidden = shaped(slot_count, hidden, dtype=f32)
    act, gate_factor, up_factor = kernel(
        forward_kernel,
        (shaped(slot_count, hidden), wide_hidden, wide_hidden),
        "forward",
        *rows,
        gate_proj[0],
        up_proj[0],
        scalar=place,
        flops=1 << 31,
    )
    half = slot_count // 2
    forward, backward = ring_pairs("tp")
    gate_delta, up_delta, far = kernel(
        delta_kernel,
        (shaped(slot_count, hidden), shaped(slot_count, hidden), shaped(slot_count, span)),
        "delta",
        *grads,
        down_proj[0],
        gate_proj[0],
        up_proj[0],
        gate_factor,
        up_factor,
        scalar=place,
    )
    from_left = lax.ppermute(far[:half], "tp", forward)
    from_right = lax.ppermute(far[half:], "tp", backward)
    part = shaped(slot_count, span, dtype=f32)
    for_right, for_left, for_own = kernel(
        partial_kernel,
        (part, part, part),
        "partial",
        gate_delta,
        up_delta,
        gate_proj[0],
        up_proj[0],
        scalar=place,
        flops=1 << 30,
    )
    to_right, to_left = kernel(
        relay_kernel,
        (shaped(slot_count, span), shaped(slot_count, span)),
        "relay",
        for_right,
        for_left,
        from_left,
        from_right,
    )
    got_left = lax.ppermute(to_right, "tp", forward)
    got_right = lax.ppermute(to_left, "tp", backward)
    summed = kernel(
        gather_kernel,
        packed_shape,
        "gather",
        for_own,
        got_left,
        got_right,
        scratch=(pack_scratch,),
    )
    returned = lax.all_to_all(summed, "sp", 0, 0, tiled=True)
    token_part = kernel(
        combine_kernel,
        shaped(tok_rows, span),
        "combine",
        returned,
        pick0,
        pick1,
        scratch=(pack_scratch, pltpu.VMEM((slot_count, span), bf16)),
    )
    token_grad = sent_to_all(token_part, "tp")
    wide = shaped(2 * tok_rows, channels, dtype=f32)
    edges = shaped(5 * EDGE, channels, dtype=f32)
    piece = embedding_width // shards
    branch_gate_grad, local, prod, sent, low, high = kernel(
        branch_kernel,
        (
            shaped(tok_rows, channels),
            wide,
            wide,
            shaped(shards, piece + 8, channels),
            edges,
            edges,
        ),
        "branch",
        token_grad,
        mid,
        inv_rms,
        out_grad,
        out_proj,
        summed_states,
        gelu_value,
        gelu_slope,
        decay_factors.reshape(2 * tok_rows, channels),
        mixed_b,
        first_edge,
        last_edge,
        scratch=(pltpu.VMEM((tok_rows, channels), f32),),
    )
    ring_on = [(i, i + 1) for i in range(shards - 1)]
    ring_back = [(target, source) for source, target in ring_on]
    got = lax.all_to_all(sent, "sp", 0, 0, tiled=True)
    after = lax.ppermute(low, "sp", ring_back)
    before = lax.ppermute(high, "sp", ring_on)
    rows, grads, act, gate_delta, up_delta, _ = lax.optimization_barrier(
        (rows, grads, act, gate_delta, up_delta, sent)
    )
    gate_grad, up_grad, down_grad = kernel(
        weights_kernel,
        (
            shaped(embedding_width, hidden),
            shaped(embedding_width, hidden),
            shaped(hidden, embedding_width),
        ),
        "weights",
        *rows,
        *grads,
        act,
        gate_delta,
        up_delta,
        scalar=place,
        flops=1 << 31,
    )
    here = lax.axis_index("sp").astype(jnp.int32).reshape(1)
    input_grad, proj_grad_t = kernel(
        tail_kernel,
        (shaped(tok_rows, channels), shaped(piece, channels, dtype=f32)),
        "tail",
        got,
        local,
        prod,
        drive_coef.reshape(2 * tok_rows, channels),
        rate_coef.reshape(2 * tok_rows, channels),
        input_coef.reshape(2 * tok_rows, channels),
        after,
        before,
        rate_blocks,
        input_blocks,
        conv_taps.astype(f32).reshape(-1, channels),
        scalar=here,
        scratch=[pltpu.VMEM((tok_rows + EDGE, channels), f32)] * 2
        + [pltpu.VMEM((8 * shards, channels), f32)],
    )
    return (
        gate_grad[None],
        up_grad[None],
        down_grad[None],
        proj_grad_t,
        input_grad,
        branch_gate_grad,
    )


def solution(mesh):
    in_specs = (
        P("sp", None),
        P("sp", None),
        P("sp", None),
        P("sp", None),
        P("sp", None, "tp"),
        P("sp", None, "tp"),
        P("sp", "tp", None),
        P("tp", None),
        P("sp", "tp"),
        P(None, "sp", "tp"),
        P(None, "sp", "tp"),
        P(None, "tp", None, None),
        P(None, "tp", None, None),
        P(None, "tp"),
        P(None, "sp", "tp"),
        P(None, None, "tp"),
    )
    out_specs = (
        P("sp", None, "tp"),
        P("sp", None, "tp"),
        P("sp", "tp", None),
        P("sp", "tp"),
        P("sp", "tp"),
        P("sp", "tp"),
    )
    return jax.shard_map(
        on_device, mesh=mesh, in_specs=in_specs, out_specs=out_specs, check_vma=False
    )
```

```python
import jax
import jax.numpy as jnp
from jax import lax
from jax.experimental import pallas as pl
from jax.experimental.pallas import tpu as pltpu
from jax.sharding import PartitionSpec as P

RATE_SCALE = 8.0
CLAMP_LIMIT = 7.0
SHARPNESS = 1.702
NORM_EPSILON = 1e-06
STATE_FLOOR = 0.001
GELU_CUBIC = 0.044715
GELU_SCALE = 0.7978845608028654
LANES = 128


def ring_pairs(axis):
    count = lax.axis_size(axis)
    forward = [(i, (i + 1) % count) for i in range(count)]
    return forward, [(target, source) for source, target in forward]


def ring_blocks(x, axis):
    forward, backward = ring_pairs(axis)
    half = x.shape[0] // 2
    left = lax.ppermute(x, axis, forward)
    right = lax.ppermute(x, axis, backward)
    left_cut, right_cut = left[:half], right[half:]
    far_top = lax.ppermute(left_cut, axis, forward)
    far_bottom = lax.ppermute(right_cut, axis, backward)
    return x, right, far_top, far_bottom, left


def gelu_parts(values):
    inside = GELU_SCALE * (values + GELU_CUBIC * values * values * values)
    tangent = jnp.tanh(inside)
    result = 0.5 * values * (1.0 + tangent)
    slope_value = 0.5 * (1.0 + tangent) + 0.5 * values * (1.0 - tangent * tangent) * GELU_SCALE * (
        1.0 + 3.0 * GELU_CUBIC * values * values
    )
    return (result, slope_value)


SEGMENTS = 8
EDGE = 8


def over_segments(a_rows, b_rows, order):
    carry, factor = jnp.zeros_like(a_rows[:1]), jnp.ones_like(a_rows[:1])
    carries, factors = [None] * SEGMENTS, [None] * SEGMENTS
    for s in order:
        carries[s], factors[s] = carry, factor
        a, b = a_rows[s : s + 1], b_rows[s : s + 1]
        carry, factor = a * carry + b, a * factor
    return jnp.concatenate(carries), jnp.concatenate(factors), factor, carry


def scan_side(seed_ref, decay_ref, local_ref, prod_ref, base, rows, reverse):
    step = rows // SEGMENTS

    def at(i):
        return pl.ds(base + i, SEGMENTS, stride=step)

    order = list(range(step))[::-1] if reverse else list(range(step))
    value = factor = last = None
    for i in order:
        seed = seed_ref[pl.ds(i, SEGMENTS, stride=step), :]
        value = seed if value is None else seed + last * value
        factor = jnp.ones_like(seed) if factor is None else factor * last
        local_ref[at(i), :] = value
        prod_ref[at(i), :] = factor
        last = decay_ref[at(i), :]
    segs = range(SEGMENTS)[::-1] if reverse else range(SEGMENTS)
    carries, factors, whole_factor, whole_value = over_segments(
        factor * last, value * last, segs
    )
    for i in range(step):
        prod = prod_ref[at(i), :]
        local_ref[at(i), :] = local_ref[at(i), :] + prod * carries
        prod_ref[at(i), :] = prod * factors
    return whole_factor, whole_value


def branch_kernel(
    token_ref,
    mid_ref,
    inv_ref,
    cot_ref,
    out_proj_ref,
    states_ref,
    gelu_ref,
    slope_ref,
    decay_ref,
    mixed_ref,
    first_ref,
    last_ref,
    gate_out_ref,
    local_ref,
    prod_ref,
    send_ref,
    low_ref,
    high_ref,
    seed_ref,
):
    shards = send_ref.shape[0]
    share = shards // token_ref.shape[0]
    piece = token_ref.shape[2] // share
    groups, rows, span = token_ref.shape
    inv = inv_ref[...]
    total = jnp.zeros_like(inv)
    for k in range(groups):
        cols = slice(k * span, (k + 1) * span)
        normed = mid_ref[:, cols].astype(jnp.float32) * inv
        total = total + jnp.sum(
            token_ref[k].astype(jnp.float32) * normed, axis=1, keepdims=True
        )
    mean = total / (groups * span)
    branch = jnp.zeros(states_ref.shape, jnp.float32)
    for k in range(groups):
        cols = slice(k * span, (k + 1) * span)
        normed = mid_ref[:, cols].astype(jnp.float32) * inv
        grad = (
            cot_ref[:, cols].astype(jnp.float32)
            + inv * (token_ref[k].astype(jnp.float32) - normed * mean)
        ).astype(jnp.bfloat16)
        branch = branch + last_dims(grad, out_proj_ref[:, cols])
        proj = first_dims(grad, mixed_ref[...]).astype(jnp.bfloat16)
        send_ref[k * share : (k + 1) * share, :piece, :] = proj.reshape(share, piece, LANES)
    gate_out_ref[...] = (branch * states_ref[...] * slope_ref[...]).astype(jnp.bfloat16)
    seed_ref[...] = branch * gelu_ref[...]
    later = scan_side(seed_ref, decay_ref, local_ref, prod_ref, 0, rows, True)
    earlier = scan_side(seed_ref, decay_ref, local_ref, prod_ref, rows, rows, False)
    maps = jnp.concatenate([*later, *earlier])
    high_part = maps.astype(jnp.bfloat16)
    low_part = (maps - high_part.astype(jnp.float32)).astype(jnp.bfloat16)
    pair = jnp.concatenate(
        [high_part.astype(jnp.float32), low_part.astype(jnp.float32)]
    ).astype(jnp.bfloat16)
    send_ref[:, piece:, :] = jnp.broadcast_to(pair[None], (shards, *pair.shape))
    low_ref[:EDGE] = local_ref[:EDGE]
    low_ref[EDGE : 2 * EDGE] = prod_ref[:EDGE]
    low_ref[2 * EDGE :] = first_ref[...]
    high_ref[:EDGE] = local_ref[2 * rows - EDGE :]
    high_ref[EDGE : 2 * EDGE] = prod_ref[2 * rows - EDGE :]
    high_ref[2 * EDGE :] = last_ref[...]


def folded(maps_ref, which, kept, reverse):
    count = maps_ref.shape[0] // 8
    step = count // SEGMENTS
    lead = step * lax.broadcasted_iota(jnp.int32, (SEGMENTS, LANES), 0)
    value = jnp.zeros((SEGMENTS, LANES), jnp.float32)
    factor = jnp.ones((SEGMENTS, LANES), jnp.float32)
    for i in range(step)[::-1] if reverse else range(step):
        use = kept(lead + i)
        a, b = (
            maps_ref[pl.ds(8 * i + q, SEGMENTS, stride=8 * step), :]
            + maps_ref[pl.ds(8 * i + q + 4, SEGMENTS, stride=8 * step), :]
            for q in (which, which + 1)
        )
        a, b = jnp.where(use, a, 1.0), jnp.where(use, b, 0.0)
        value, factor = a * value + b, factor * a
    carry = jnp.zeros((1, LANES), jnp.float32)
    for s in range(SEGMENTS)[::-1] if reverse else range(SEGMENTS):
        carry = factor[s : s + 1] * carry + value[s : s + 1]
    return carry


def tail_kernel(
    here_ref,
    got_ref,
    local_ref,
    prod_ref,
    drive_ref,
    rate_ref,
    input_ref,
    after_ref,
    before_ref,
    rate_w_ref,
    input_w_ref,
    taps_ref,
    out_ref,
    proj_ref,
    later_ref,
    earlier_ref,
    maps_ref,
):
    here = here_ref[0]
    piece = proj_ref.shape[0]
    proj_ref[...] = jnp.sum(got_ref[:, :piece, :].astype(jnp.float32), axis=0)
    maps_ref[...] = got_ref[:, piece:, :].astype(jnp.float32).reshape(maps_ref.shape)
    rows = out_ref.shape[0]
    reach = taps_ref.shape[0] // 2 - 1

    def spread(side, adjoint, drive, rate, inp):
        def back(coef, w_ref):
            return lax.dot_general(
                (adjoint * coef).astype(jnp.bfloat16),
                w_ref[side],
                (((1,), (1,)), ((), ())),
                preferred_element_type=jnp.float32,
            )

        return adjoint * drive + back(rate, rate_w_ref) + back(inp, input_w_ref)

    def main(side, inflow):
        own = slice(side * rows, (side + 1) * rows)
        adjoint = local_ref[own] + prod_ref[own] * inflow
        return spread(side, adjoint, drive_ref[own], rate_ref[own], input_ref[own])

    def edge(side, ref, inflow):
        part = [ref[k * EDGE : (k + 1) * EDGE] for k in range(5)]
        return spread(side, part[0] + part[1] * inflow, *part[2:])

    later_ref[:rows] = main(0, folded(maps_ref, 0, lambda j: j > here, True))
    later_ref[rows:] = edge(0, after_ref, folded(maps_ref, 0, lambda j: j > here + 1, True))
    earlier_ref[:EDGE] = edge(
        1, before_ref, folded(maps_ref, 2, lambda j: j < here - 1, False)
    )
    earlier_ref[EDGE:] = main(1, folded(maps_ref, 2, lambda j: j < here, False))
    total = jnp.zeros((rows, LANES), jnp.float32)
    for k in range(reach + 1):
        up, down = reach - k, EDGE - reach + k
        total = total + taps_ref[k : k + 1] * later_ref[up : up + rows]
        total = (
            total
            + taps_ref[reach + 1 + k : reach + 2 + k] * earlier_ref[down : down + rows]
        )
    out_ref[...] = total.astype(jnp.bfloat16)


ROOM_PAD = 40
VMEM_ROOM = 24 << 20


def row_of(slot, part, parts):
    return slot * parts + part


def pack_rows(value, scratch_ref, out_ref, room):
    shards = out_ref.shape[0]
    parts = value.shape[1] // LANES
    for r in range(room):
        for c in range(parts):
            scratch_ref[pl.ds(row_of(r, c, parts), shards, stride=ROOM_PAD), :] = value[
                r * shards : (r + 1) * shards, c * LANES : (c + 1) * LANES
            ]
    for extra in range(room * parts, ROOM_PAD):
        scratch_ref[pl.ds(extra, shards, stride=ROOM_PAD), :] = jnp.zeros(
            (shards, LANES), jnp.float32
        )
    out_ref[...] = scratch_ref[...].reshape(out_ref.shape).astype(jnp.bfloat16)


def unpack_rows(in_ref, scratch_ref, out_ref, room):
    shards = in_ref.shape[0]
    parts = out_ref.shape[1] // LANES
    scratch_ref[...] = in_ref[...].astype(jnp.float32).reshape(scratch_ref.shape)
    for r in range(room):
        for c in range(parts):
            out_ref[r * shards : (r + 1) * shards, c * LANES : (c + 1) * LANES] = scratch_ref[
                pl.ds(row_of(r, c, parts), shards, stride=ROOM_PAD), :
            ].astype(jnp.bfloat16)


def first_dims(a, b):
    return lax.dot_general(a, b, (((0,), (0,)), ((), ())), preferred_element_type=jnp.float32)


def last_dims(a, b):
    return lax.dot_general(a, b, (((1,), (1,)), ((), ())), preferred_element_type=jnp.float32)


def plain(a, b):
    return jnp.dot(a, b, preferred_element_type=jnp.float32)


def route_kernel(
    place_ref, ids_ref, mid_ref, packed_ref, inv_ref, pick0_ref, pick1_ref, scratch_ref
):
    rows, width = mid_ref.shape
    shards = packed_ref.shape[0]
    slots = pick0_ref.shape[0]
    span = packed_ref.shape[1] * LANES // (slots // shards) // LANES * LANES
    ids = ids_ref[...]
    experts = lax.broadcasted_iota(jnp.int32, (shards, rows), 0)
    hits = [ids[k : k + 1] == experts for k in range(2)]
    named = (hits[0] | hits[1]).astype(jnp.bfloat16)
    earlier = (
        lax.broadcasted_iota(jnp.int32, (rows, rows), 0)
        < lax.broadcasted_iota(jnp.int32, (rows, rows), 1)
    ).astype(jnp.bfloat16)
    ranks = plain(named, earlier)
    tall = lax.broadcasted_iota(jnp.int32, (slots, rows), 0)
    picks = []
    for k, ref in enumerate((pick0_ref, pick1_ref)):
        rank = jnp.sum(jnp.where(hits[k], ranks, 0.0), axis=0, keepdims=True)
        target = rank.astype(jnp.int32) * shards + ids[k : k + 1]
        pick = (tall == target).astype(jnp.bfloat16)
        ref[...] = pick
        picks.append(pick)
    total = jnp.zeros((rows, 1), jnp.float32)
    step = 512
    for c in range(width // step):
        part = mid_ref[:, c * step : (c + 1) * step].astype(jnp.float32)
        total = total + jnp.sum(part * part, axis=1, keepdims=True)
    inv = lax.rsqrt(total / width + NORM_EPSILON)
    inv_ref[...] = inv
    own = mid_ref[:, pl.ds(pl.multiple_of(place_ref[0] * span, LANES), span)]
    normed = (own.astype(jnp.float32) * inv).astype(jnp.bfloat16)
    pack_rows(plain(picks[0] + picks[1], normed), scratch_ref, packed_ref, slots // shards)


def weigh_kernel(place_ref, weights_ref, cot_ref, pick0_ref, pick1_ref, packed_ref, scratch_ref):
    shards = packed_ref.shape[0]
    slots = pick0_ref.shape[0]
    span = packed_ref.shape[1] * LANES // (slots // shards) // LANES * LANES
    own = cot_ref[:, pl.ds(pl.multiple_of(place_ref[0] * span, LANES), span)]
    weight = jnp.sum(
        pick0_ref[...].astype(jnp.float32) * weights_ref[0:1]
        + pick1_ref[...].astype(jnp.float32) * weights_ref[1:2],
        axis=1,
        keepdims=True,
    )
    total = plain(pick0_ref[...] + pick1_ref[...], own) * weight
    pack_rows(total, scratch_ref, packed_ref, slots // shards)


def unpack_kernel(in_ref, out_ref, scratch_ref):
    unpack_rows(in_ref, scratch_ref, out_ref, out_ref.shape[0] // in_ref.shape[0])


def offsets(place_ref, groups, span):
    return [
        pl.multiple_of(lax.rem(place_ref[0] + k, groups) * span, span) for k in range(groups)
    ]


def forward_kernel(
    place_ref,
    own_ref,
    right_ref,
    top_ref,
    bottom_ref,
    left_ref,
    gate_ref,
    up_ref,
    act_ref,
    gate_factor_ref,
    up_factor_ref,
):
    _, span = top_ref.shape
    at = offsets(place_ref, gate_ref.shape[0] // span, span)
    far = jnp.concatenate([top_ref[...], bottom_ref[...]])

    def pre(w_ref):
        total = plain(own_ref[...], w_ref[pl.ds(at[0], span), :])
        total = total + plain(right_ref[...], w_ref[pl.ds(at[1], span), :])
        total = total + plain(left_ref[...], w_ref[pl.ds(at[3], span), :])
        return total + plain(far, w_ref[pl.ds(at[2], span), :])

    gate_pre = pre(gate_ref)
    up_pre = pre(up_ref)
    gate = jnp.minimum(gate_pre, CLAMP_LIMIT)
    up_one = jnp.clip(up_pre, -CLAMP_LIMIT, CLAMP_LIMIT) + 1.0
    sig = jax.nn.sigmoid(SHARPNESS * gate)
    swish = gate * sig
    act_ref[...] = (up_one * swish).astype(jnp.bfloat16)
    gate_factor_ref[...] = jnp.where(
        gate_pre < CLAMP_LIMIT, up_one * (sig + SHARPNESS * swish * (1.0 - sig)), 0.0
    )
    up_factor_ref[...] = jnp.where(jnp.abs(up_pre) < CLAMP_LIMIT, swish, 0.0)


def near_kernel(place_ref, own_ref, right_ref, left_ref, down_ref, total_ref):
    span = own_ref.shape[1]
    at = offsets(place_ref, down_ref.shape[1] // span, span)
    total = last_dims(own_ref[...], down_ref[:, pl.ds(at[0], span)])
    total = total + last_dims(right_ref[...], down_ref[:, pl.ds(at[1], span)])
    total_ref[...] = total + last_dims(left_ref[...], down_ref[:, pl.ds(at[3], span)])


def delta_kernel(
    place_ref,
    near_ref,
    top_ref,
    bottom_ref,
    down_ref,
    gate_ref,
    up_ref,
    gate_factor_ref,
    up_factor_ref,
    gate_delta_ref,
    up_delta_ref,
    far_top_ref,
    far_bottom_ref,
):
    half, span = top_ref.shape
    at = offsets(place_ref, gate_ref.shape[0] // span, span)
    far = jnp.concatenate([top_ref[...], bottom_ref[...]])
    act_grad = near_ref[...] + last_dims(far, down_ref[:, pl.ds(at[2], span)])
    gate_delta = (act_grad * gate_factor_ref[...]).astype(jnp.bfloat16)
    up_delta = (act_grad * up_factor_ref[...]).astype(jnp.bfloat16)
    gate_delta_ref[...] = gate_delta
    up_delta_ref[...] = up_delta
    out = (
        last_dims(gate_delta, gate_ref[pl.ds(at[2], span), :])
        + last_dims(up_delta, up_ref[pl.ds(at[2], span), :])
    ).astype(jnp.bfloat16)
    far_top_ref[...] = out[:half]
    far_bottom_ref[...] = out[half:]


def partial_kernel(place_ref, gate_delta_ref, up_delta_ref, gate_ref, up_ref, *out_refs):
    span = out_refs[0].shape[1]
    at = offsets(place_ref, gate_ref.shape[0] // span, span)
    for k, ref in zip((1, 3, 0), out_refs):
        ref[...] = last_dims(gate_delta_ref[...], gate_ref[pl.ds(at[k], span), :]) + last_dims(
            up_delta_ref[...], up_ref[pl.ds(at[k], span), :]
        )


def relay_kernel(right_ref, left_ref, from_left_ref, from_right_ref, to_right_ref, to_left_ref):
    half = from_left_ref.shape[0]
    bf = jnp.bfloat16
    to_right_ref[:half] = (right_ref[:half] + from_left_ref[...].astype(jnp.float32)).astype(bf)
    to_right_ref[half:] = right_ref[half:].astype(bf)
    to_left_ref[:half] = left_ref[:half].astype(bf)
    to_left_ref[half:] = (left_ref[half:] + from_right_ref[...].astype(jnp.float32)).astype(bf)


def gather_kernel(own_ref, from_left_ref, from_right_ref, packed_ref, scratch_ref):
    total = (
        own_ref[...]
        + from_left_ref[...].astype(jnp.float32)
        + from_right_ref[...].astype(jnp.float32)
    )
    pack_rows(total, scratch_ref, packed_ref, total.shape[0] // packed_ref.shape[0])


def combine_kernel(in_ref, pick0_ref, pick1_ref, out_ref, scratch_ref, rows_ref):
    unpack_rows(in_ref, scratch_ref, rows_ref, rows_ref.shape[0] // in_ref.shape[0])
    total = first_dims(pick0_ref[...] + pick1_ref[...], rows_ref[...]).astype(jnp.bfloat16)
    for k in range(out_ref.shape[0]):
        out_ref[k] = total


def weights_kernel(
    place_ref,
    r_own_ref,
    r_right_ref,
    r_top_ref,
    r_bottom_ref,
    r_left_ref,
    g_own_ref,
    g_right_ref,
    g_top_ref,
    g_bottom_ref,
    g_left_ref,
    act_ref,
    gate_delta_ref,
    up_delta_ref,
    gate_out_ref,
    up_out_ref,
    down_out_ref,
):
    _, span = r_top_ref.shape
    at = offsets(place_ref, gate_out_ref.shape[0] // span, span)
    rows = (r_own_ref, r_right_ref, (r_top_ref, r_bottom_ref), r_left_ref)
    grads = (g_own_ref, g_right_ref, (g_top_ref, g_bottom_ref), g_left_ref)
    bf = jnp.bfloat16

    def whole(block):
        if isinstance(block, tuple):
            return jnp.concatenate([part[...] for part in block])
        return block[...]

    for k in range(4):
        row = whole(rows[k])
        gate_out_ref[pl.ds(at[k], span), :] = first_dims(row, gate_delta_ref[...]).astype(bf)
        up_out_ref[pl.ds(at[k], span), :] = first_dims(row, up_delta_ref[...]).astype(bf)
        down_out_ref[:, pl.ds(at[k], span)] = first_dims(act_ref[...], whole(grads[k])).astype(bf)


def on_device(
    mid,
    out_grad,
    expert_ids,
    route_weights,
    gate_proj,
    up_proj,
    down_proj,
    out_proj,
    branch_gate,
    conv_out,
    prior_state,
    rate_gate_w,
    input_gate_w,
    decay_param,
    decay_jump,
    conv_taps,
):
    tok_rows, embedding_width = mid.shape
    shards = lax.axis_size("sp")
    groups = lax.axis_size("tp")
    local_experts = gate_proj.shape[0]
    experts_all = local_experts * shards
    top_count = expert_ids.shape[1]
    expert_room = 3 * top_count * tok_rows // (2 * experts_all)
    slot_count = experts_all * expert_room
    span = embedding_width // groups
    hidden = gate_proj.shape[2]
    bf16, f32 = (jnp.bfloat16, jnp.float32)

    def shaped(*dims, dtype=bf16):
        return jax.ShapeDtypeStruct(dims, dtype)

    vmem = pl.BlockSpec(memory_space=pltpu.VMEM)
    smem = pl.BlockSpec(memory_space=pltpu.SMEM)

    def kernel(body, outs, *args, scalar=None, scratch=(), flops=0):
        lead = () if scalar is None else (scalar,)
        return pl.pallas_call(
            body,
            out_shape=outs,
            in_specs=[smem] * len(lead) + [vmem] * len(args),
            scratch_shapes=list(scratch),
            compiler_params=pltpu.CompilerParams(vmem_limit_bytes=VMEM_ROOM),
            cost_estimate=pl.CostEstimate(flops=flops, transcendentals=0, bytes_accessed=0),
        )(*lead, *args)

    packed_shape = shaped(shards, ROOM_PAD, LANES)
    pack_scratch = pltpu.VMEM((shards * ROOM_PAD, LANES), f32)
    place = lax.axis_index("tp").astype(jnp.int32).reshape(1)
    pick_shape = shaped(slot_count, tok_rows)
    sent_rows, inv_rms, pick0, pick1 = kernel(
        route_kernel,
        (packed_shape, shaped(tok_rows, 1, dtype=f32), pick_shape, pick_shape),
        expert_ids.T,
        mid,
        scalar=place,
        scratch=(pack_scratch,),
    )
    sent_grad = kernel(
        weigh_kernel,
        packed_shape,
        route_weights.T,
        out_grad,
        pick0,
        pick1,
        scalar=place,
        scratch=(pack_scratch,),
        flops=1 << 28,
    )
    heads_local = rate_gate_w.shape[1]
    head_width = rate_gate_w.shape[2]
    channels = heads_local * head_width

    def on_diagonal(w):
        return jnp.concatenate(
            [
                jnp.pad(
                    w[:, h],
                    ((0, 0), (0, 0), (h * head_width, channels - (h + 1) * head_width)),
                )
                for h in range(heads_local)
            ],
            axis=1,
        )

    rate_blocks, input_blocks = on_diagonal(rate_gate_w), on_diagonal(input_gate_w)

    def gate_of(blocks):
        return jax.nn.sigmoid(
            jnp.einsum("stc,scd->std", conv_out, blocks, preferred_element_type=jnp.float32)
        )

    rate_gate, input_gate = gate_of(rate_blocks), gate_of(input_blocks)
    decay_rate = jax.nn.softplus(-decay_param)[:, None, :]
    log_decay = -RATE_SCALE * rate_gate * decay_rate + decay_jump
    decay_factors = jnp.exp(log_decay)
    squared = jnp.exp(2.0 * log_decay)
    norm_factor = jnp.sqrt(STATE_FLOOR - jnp.expm1(2.0 * log_decay))
    conv_full = conv_out.astype(jnp.float32)
    drive_term = input_gate * conv_full
    decayed = decay_factors * prior_state
    states = decayed + norm_factor * drive_term
    summed_states = states[0] + states[1]
    gelu_value, gelu_slope = gelu_parts(branch_gate.astype(jnp.float32))
    mixed_b = (summed_states * gelu_value).astype(jnp.bfloat16)
    rate_coef = (
        (decayed - drive_term * squared / norm_factor)
        * (-RATE_SCALE * decay_rate)
        * rate_gate
        * (1.0 - rate_gate)
    )
    drive_coef = norm_factor * input_gate
    input_coef = norm_factor * conv_full * input_gate * (1.0 - input_gate)
    first_edge = jnp.concatenate([c[0, :EDGE] for c in (drive_coef, rate_coef, input_coef)])
    last_edge = jnp.concatenate([c[1, -EDGE:] for c in (drive_coef, rate_coef, input_coef)])
    (
        sent_grad,
        decay_factors,
        summed_states,
        gelu_value,
        gelu_slope,
        mixed_b,
        rate_coef,
        drive_coef,
        input_coef,
        first_edge,
        last_edge,
    ) = lax.optimization_barrier(
        (
            sent_grad,
            decay_factors,
            summed_states,
            gelu_value,
            gelu_slope,
            mixed_b,
            rate_coef,
            drive_coef,
            input_coef,
            first_edge,
            last_edge,
        )
    )

    def unpacked(x):
        return kernel(unpack_kernel, shaped(slot_count, span), x, scratch=(pack_scratch,))

    got_rows = lax.all_to_all(sent_rows, "sp", 0, 0, tiled=True)
    rows = ring_blocks(unpacked(got_rows), "tp")
    got_grad = lax.all_to_all(sent_grad, "sp", 0, 0, tiled=True)
    grads = ring_blocks(unpacked(got_grad), "tp")
    wide_hidden = shaped(slot_count, hidden, dtype=f32)
    act, gate_factor, up_factor = kernel(
        forward_kernel,
        (shaped(slot_count, hidden), wide_hidden, wide_hidden),
        *rows,
        gate_proj[0],
        up_proj[0],
        scalar=place,
        flops=1 << 31,
    )
    half = slot_count // 2
    forward, backward = ring_pairs("tp")
    near = kernel(
        near_kernel,
        wide_hidden,
        grads[0],
        grads[1],
        grads[4],
        down_proj[0],
        scalar=place,
        flops=1 << 30,
    )
    gate_delta, up_delta, far_top, far_bottom = kernel(
        delta_kernel,
        (
            shaped(slot_count, hidden),
            shaped(slot_count, hidden),
            shaped(half, span),
            shaped(half, span),
        ),
        near,
        grads[2],
        grads[3],
        down_proj[0],
        gate_proj[0],
        up_proj[0],
        gate_factor,
        up_factor,
        scalar=place,
    )
    from_left = lax.ppermute(far_top, "tp", forward)
    from_right = lax.ppermute(far_bottom, "tp", backward)
    part = shaped(slot_count, span, dtype=f32)
    for_right, for_left, for_own = kernel(
        partial_kernel,
        (part, part, part),
        gate_delta,
        up_delta,
        gate_proj[0],
        up_proj[0],
        scalar=place,
        flops=1 << 30,
    )
    to_right, to_left = kernel(
        relay_kernel,
        (shaped(slot_count, span), shaped(slot_count, span)),
        for_right,
        for_left,
        from_left,
        from_right,
    )
    got_left = lax.ppermute(to_right, "tp", forward)
    got_right = lax.ppermute(to_left, "tp", backward)
    summed = kernel(
        gather_kernel, packed_shape, for_own, got_left, got_right, scratch=(pack_scratch,)
    )
    returned = lax.all_to_all(summed, "sp", 0, 0, tiled=True)
    token_copies = kernel(
        combine_kernel,
        shaped(groups, tok_rows, span),
        returned,
        pick0,
        pick1,
        scratch=(pack_scratch, pltpu.VMEM((slot_count, span), bf16)),
    )
    token_grad = lax.all_to_all(token_copies, "tp", 0, 0, tiled=True)
    wide = shaped(2 * tok_rows, channels, dtype=f32)
    edges = shaped(5 * EDGE, channels, dtype=f32)
    piece = embedding_width // shards
    branch_gate_grad, local, prod, sent, low, high = kernel(
        branch_kernel,
        (
            shaped(tok_rows, channels),
            wide,
            wide,
            shaped(shards, piece + 8, channels),
            edges,
            edges,
        ),
        token_grad,
        mid,
        inv_rms,
        out_grad,
        out_proj,
        summed_states,
        gelu_value,
        gelu_slope,
        decay_factors.reshape(2 * tok_rows, channels),
        mixed_b,
        first_edge,
        last_edge,
        scratch=(pltpu.VMEM((tok_rows, channels), f32),),
    )
    ring_on = [(i, i + 1) for i in range(shards - 1)]
    ring_back = [(target, source) for source, target in ring_on]
    got = lax.all_to_all(sent, "sp", 0, 0, tiled=True)
    after = lax.ppermute(low, "sp", ring_back)
    before = lax.ppermute(high, "sp", ring_on)
    gate_grad, up_grad, down_grad = kernel(
        weights_kernel,
        (
            shaped(embedding_width, hidden),
            shaped(embedding_width, hidden),
            shaped(hidden, embedding_width),
        ),
        *rows,
        *grads,
        act,
        gate_delta,
        up_delta,
        scalar=place,
        flops=1 << 31,
    )
    here = lax.axis_index("sp").astype(jnp.int32).reshape(1)
    input_grad, proj_grad_t = kernel(
        tail_kernel,
        (shaped(tok_rows, channels), shaped(piece, channels, dtype=f32)),
        got,
        local,
        prod,
        drive_coef.reshape(2 * tok_rows, channels),
        rate_coef.reshape(2 * tok_rows, channels),
        input_coef.reshape(2 * tok_rows, channels),
        after,
        before,
        rate_blocks,
        input_blocks,
        conv_taps.astype(f32).reshape(-1, channels),
        scalar=here,
        scratch=[pltpu.VMEM((tok_rows + EDGE, channels), f32)] * 2
        + [pltpu.VMEM((8 * shards, channels), f32)],
    )
    return (
        gate_grad[None],
        up_grad[None],
        down_grad[None],
        proj_grad_t,
        input_grad,
        branch_gate_grad,
    )


def solution(mesh):
    in_specs = (
        P("sp", None),
        P("sp", None),
        P("sp", None),
        P("sp", None),
        P("sp", None, "tp"),
        P("sp", None, "tp"),
        P("sp", "tp", None),
        P("tp", None),
        P("sp", "tp"),
        P(None, "sp", "tp"),
        P(None, "sp", "tp"),
        P(None, "tp", None, None),
        P(None, "tp", None, None),
        P(None, "tp"),
        P(None, "sp", "tp"),
        P(None, None, "tp"),
    )
    out_specs = (
        P("sp", None, "tp"),
        P("sp", None, "tp"),
        P("sp", "tp", None),
        P("sp", "tp"),
        P("sp", "tp"),
        P("sp", "tp"),
    )

    return jax.shard_map(
        on_device, mesh=mesh, in_specs=in_specs, out_specs=out_specs, check_vma=False
    )
```

```python
import jax
import jax.numpy as jnp
from jax import lax
from jax.experimental import pallas as pl
from jax.experimental.pallas import tpu as pltpu
from jax.sharding import PartitionSpec as P

RATE_SCALE = 8.0
CLAMP_LIMIT = 7.0
SHARPNESS = 1.702
NORM_EPSILON = 1e-06
STATE_FLOOR = 0.001
GELU_CUBIC = 0.044715
GELU_SCALE = 0.7978845608028654
LANES = 128


def ring_pairs(axis):
    count = lax.axis_size(axis)
    forward = [(i, (i + 1) % count) for i in range(count)]
    return forward, [(target, source) for source, target in forward]


def ring_blocks(top, bottom, axis):
    forward, backward = ring_pairs(axis)
    left_top = lax.ppermute(top, axis, forward)
    right_bottom = lax.ppermute(bottom, axis, backward)
    left_bottom = lax.ppermute(bottom, axis, forward)
    right_top = lax.ppermute(top, axis, backward)
    far_top = lax.ppermute(left_top, axis, forward)
    far_bottom = lax.ppermute(right_bottom, axis, backward)
    corner = left_top[:8, :LANES] + right_bottom[:8, :LANES]
    near = (top, bottom, right_top, right_bottom, left_top, left_bottom)
    return near, (far_top, far_bottom), corner


def gelu_parts(values):
    inside = GELU_SCALE * (values + GELU_CUBIC * values * values * values)
    tangent = jnp.tanh(inside)
    result = 0.5 * values * (1.0 + tangent)
    slope_value = 0.5 * (1.0 + tangent) + 0.5 * values * (1.0 - tangent * tangent) * GELU_SCALE * (
        1.0 + 3.0 * GELU_CUBIC * values * values
    )
    return (result, slope_value)


SEGMENTS = 8
EDGE = 8


def over_segments(a_rows, b_rows, order):
    carry, factor = jnp.zeros_like(a_rows[:1]), jnp.ones_like(a_rows[:1])
    carries, factors = [None] * SEGMENTS, [None] * SEGMENTS
    for s in order:
        carries[s], factors[s] = carry, factor
        a, b = a_rows[s : s + 1], b_rows[s : s + 1]
        carry, factor = a * carry + b, a * factor
    return jnp.concatenate(carries), jnp.concatenate(factors), factor, carry


def scan_side(seed_ref, decay_ref, local_ref, prod_ref, base, rows, reverse):
    step = rows // SEGMENTS

    def at(i):
        return pl.ds(base + i, SEGMENTS, stride=step)

    order = list(range(step))[::-1] if reverse else list(range(step))
    value = factor = last = None
    for i in order:
        seed = seed_ref[pl.ds(i, SEGMENTS, stride=step), :]
        value = seed if value is None else seed + last * value
        factor = jnp.ones_like(seed) if factor is None else factor * last
        local_ref[at(i), :] = value
        prod_ref[at(i), :] = factor
        last = decay_ref[at(i), :]
    segs = range(SEGMENTS)[::-1] if reverse else range(SEGMENTS)
    carries, factors, whole_factor, whole_value = over_segments(
        factor * last, value * last, segs
    )
    for i in range(step):
        prod = prod_ref[at(i), :]
        local_ref[at(i), :] = local_ref[at(i), :] + prod * carries
        prod_ref[at(i), :] = prod * factors
    return whole_factor, whole_value


def branch_kernel(
    token_ref,
    mid_ref,
    inv_ref,
    cot_ref,
    out_proj_ref,
    states_ref,
    gelu_ref,
    slope_ref,
    decay_ref,
    mixed_ref,
    first_ref,
    last_ref,
    gate_out_ref,
    local_ref,
    prod_ref,
    send_ref,
    low_ref,
    high_ref,
    seed_ref,
):
    shards = send_ref.shape[0]
    share = shards // token_ref.shape[0]
    piece = token_ref.shape[2] // share
    groups, rows, span = token_ref.shape
    inv = inv_ref[...]
    total = jnp.zeros_like(inv)
    for k in range(groups):
        cols = slice(k * span, (k + 1) * span)
        normed = mid_ref[:, cols].astype(jnp.float32) * inv
        total = total + jnp.sum(
            token_ref[k].astype(jnp.float32) * normed, axis=1, keepdims=True
        )
    mean = total / (groups * span)
    branch = jnp.zeros(states_ref.shape, jnp.float32)
    for k in range(groups):
        cols = slice(k * span, (k + 1) * span)
        normed = mid_ref[:, cols].astype(jnp.float32) * inv
        grad = (
            cot_ref[:, cols].astype(jnp.float32)
            + inv * (token_ref[k].astype(jnp.float32) - normed * mean)
        ).astype(jnp.bfloat16)
        branch = branch + last_dims(grad, out_proj_ref[:, cols])
        proj = first_dims(grad, mixed_ref[...]).astype(jnp.bfloat16)
        send_ref[k * share : (k + 1) * share, :piece, :] = proj.reshape(share, piece, LANES)
    gate_out_ref[...] = (branch * states_ref[...] * slope_ref[...]).astype(jnp.bfloat16)
    seed_ref[...] = branch * gelu_ref[...]
    later = scan_side(seed_ref, decay_ref, local_ref, prod_ref, 0, rows, True)
    earlier = scan_side(seed_ref, decay_ref, local_ref, prod_ref, rows, rows, False)
    maps = jnp.concatenate([*later, *earlier])
    high_part = maps.astype(jnp.bfloat16)
    low_part = (maps - high_part.astype(jnp.float32)).astype(jnp.bfloat16)
    pair = jnp.concatenate(
        [high_part.astype(jnp.float32), low_part.astype(jnp.float32)]
    ).astype(jnp.bfloat16)
    send_ref[:, piece:, :] = jnp.broadcast_to(pair[None], (shards, *pair.shape))
    low_ref[:EDGE] = local_ref[:EDGE]
    low_ref[EDGE : 2 * EDGE] = prod_ref[:EDGE]
    low_ref[2 * EDGE :] = first_ref[...]
    high_ref[:EDGE] = local_ref[2 * rows - EDGE :]
    high_ref[EDGE : 2 * EDGE] = prod_ref[2 * rows - EDGE :]
    high_ref[2 * EDGE :] = last_ref[...]


def folded(maps_ref, which, kept, reverse):
    count = maps_ref.shape[0] // 8
    step = count // SEGMENTS
    lead = step * lax.broadcasted_iota(jnp.int32, (SEGMENTS, LANES), 0)
    value = jnp.zeros((SEGMENTS, LANES), jnp.float32)
    factor = jnp.ones((SEGMENTS, LANES), jnp.float32)
    for i in range(step)[::-1] if reverse else range(step):
        use = kept(lead + i)
        a, b = (
            maps_ref[pl.ds(8 * i + q, SEGMENTS, stride=8 * step), :]
            + maps_ref[pl.ds(8 * i + q + 4, SEGMENTS, stride=8 * step), :]
            for q in (which, which + 1)
        )
        a, b = jnp.where(use, a, 1.0), jnp.where(use, b, 0.0)
        value, factor = a * value + b, factor * a
    carry = jnp.zeros((1, LANES), jnp.float32)
    for s in range(SEGMENTS)[::-1] if reverse else range(SEGMENTS):
        carry = factor[s : s + 1] * carry + value[s : s + 1]
    return carry


def tail_kernel(
    here_ref,
    got_ref,
    local_ref,
    prod_ref,
    drive_ref,
    rate_ref,
    input_ref,
    after_ref,
    before_ref,
    rate_w_ref,
    input_w_ref,
    taps_ref,
    out_ref,
    proj_ref,
    later_ref,
    earlier_ref,
    maps_ref,
):
    here = here_ref[0]
    piece = proj_ref.shape[0]
    proj_ref[...] = jnp.sum(got_ref[:, :piece, :].astype(jnp.float32), axis=0)
    maps_ref[...] = got_ref[:, piece:, :].astype(jnp.float32).reshape(maps_ref.shape)
    rows = out_ref.shape[0]
    reach = taps_ref.shape[0] // 2 - 1

    def spread(side, adjoint, drive, rate, inp):
        def back(coef, w_ref):
            return lax.dot_general(
                (adjoint * coef).astype(jnp.bfloat16),
                w_ref[side],
                (((1,), (1,)), ((), ())),
                preferred_element_type=jnp.float32,
            )

        return adjoint * drive + back(rate, rate_w_ref) + back(inp, input_w_ref)

    def main(side, inflow):
        own = slice(side * rows, (side + 1) * rows)
        adjoint = local_ref[own] + prod_ref[own] * inflow
        return spread(side, adjoint, drive_ref[own], rate_ref[own], input_ref[own])

    def edge(side, ref, inflow):
        part = [ref[k * EDGE : (k + 1) * EDGE] for k in range(5)]
        return spread(side, part[0] + part[1] * inflow, *part[2:])

    later_ref[:rows] = main(0, folded(maps_ref, 0, lambda j: j > here, True))
    later_ref[rows:] = edge(0, after_ref, folded(maps_ref, 0, lambda j: j > here + 1, True))
    earlier_ref[:EDGE] = edge(
        1, before_ref, folded(maps_ref, 2, lambda j: j < here - 1, False)
    )
    earlier_ref[EDGE:] = main(1, folded(maps_ref, 2, lambda j: j < here, False))
    total = jnp.zeros((rows, LANES), jnp.float32)
    for k in range(reach + 1):
        up, down = reach - k, EDGE - reach + k
        total = total + taps_ref[k : k + 1] * later_ref[up : up + rows]
        total = (
            total
            + taps_ref[reach + 1 + k : reach + 2 + k] * earlier_ref[down : down + rows]
        )
    out_ref[...] = total.astype(jnp.bfloat16)


ROOM_PAD = 40
VMEM_ROOM = 24 << 20


def row_of(slot, part, parts):
    return slot * parts + part


def pack_rows(value, scratch_ref, out_ref, room):
    shards = out_ref.shape[0]
    parts = value.shape[1] // LANES
    for r in range(room):
        for c in range(parts):
            scratch_ref[pl.ds(row_of(r, c, parts), shards, stride=ROOM_PAD), :] = value[
                r * shards : (r + 1) * shards, c * LANES : (c + 1) * LANES
            ]
    for extra in range(room * parts, ROOM_PAD):
        scratch_ref[pl.ds(extra, shards, stride=ROOM_PAD), :] = jnp.zeros(
            (shards, LANES), jnp.float32
        )
    out_ref[...] = scratch_ref[...].reshape(out_ref.shape).astype(jnp.bfloat16)


def unpack_rows(in_ref, scratch_ref, room, width):
    shards = in_ref.shape[0]
    parts = width // LANES
    scratch_ref[...] = in_ref[...].astype(jnp.float32).reshape(scratch_ref.shape)
    return jnp.concatenate(
        [
            jnp.concatenate(
                [
                    scratch_ref[pl.ds(row_of(r, c, parts), shards, stride=ROOM_PAD), :]
                    for c in range(parts)
                ],
                axis=1,
            )
            for r in range(room)
        ]
    ).astype(jnp.bfloat16)


def joined(top_ref, bottom_ref):
    return jnp.concatenate([top_ref[...], bottom_ref[...]])


def first_dims(a, b):
    return lax.dot_general(a, b, (((0,), (0,)), ((), ())), preferred_element_type=jnp.float32)


def last_dims(a, b):
    return lax.dot_general(a, b, (((1,), (1,)), ((), ())), preferred_element_type=jnp.float32)


def plain(a, b):
    return jnp.dot(a, b, preferred_element_type=jnp.float32)


def route_kernel(
    place_ref, ids_ref, mid_ref, packed_ref, inv_ref, pick0_ref, pick1_ref, scratch_ref
):
    rows, width = mid_ref.shape
    shards = packed_ref.shape[0]
    slots = pick0_ref.shape[0]
    span = packed_ref.shape[1] * LANES // (slots // shards) // LANES * LANES
    ids = ids_ref[...]
    experts = lax.broadcasted_iota(jnp.int32, (shards, rows), 0)
    hits = [ids[k : k + 1] == experts for k in range(2)]
    named = (hits[0] | hits[1]).astype(jnp.bfloat16)
    earlier = (
        lax.broadcasted_iota(jnp.int32, (rows, rows), 0)
        < lax.broadcasted_iota(jnp.int32, (rows, rows), 1)
    ).astype(jnp.bfloat16)
    ranks = plain(named, earlier)
    tall = lax.broadcasted_iota(jnp.int32, (slots, rows), 0)
    picks = []
    for k, ref in enumerate((pick0_ref, pick1_ref)):
        rank = jnp.sum(jnp.where(hits[k], ranks, 0.0), axis=0, keepdims=True)
        target = rank.astype(jnp.int32) * shards + ids[k : k + 1]
        pick = (tall == target).astype(jnp.bfloat16)
        ref[...] = pick
        picks.append(pick)
    total = jnp.zeros((rows, 1), jnp.float32)
    step = 512
    for c in range(width // step):
        part = mid_ref[:, c * step : (c + 1) * step].astype(jnp.float32)
        total = total + jnp.sum(part * part, axis=1, keepdims=True)
    inv = lax.rsqrt(total / width + NORM_EPSILON)
    inv_ref[...] = inv
    own = mid_ref[:, pl.ds(pl.multiple_of(place_ref[0] * span, LANES), span)]
    normed = (own.astype(jnp.float32) * inv).astype(jnp.bfloat16)
    pack_rows(plain(picks[0] + picks[1], normed), scratch_ref, packed_ref, slots // shards)


def weigh_kernel(place_ref, weights_ref, cot_ref, pick0_ref, pick1_ref, packed_ref, scratch_ref):
    shards = packed_ref.shape[0]
    slots = pick0_ref.shape[0]
    span = packed_ref.shape[1] * LANES // (slots // shards) // LANES * LANES
    own = cot_ref[:, pl.ds(pl.multiple_of(place_ref[0] * span, LANES), span)]
    weight = jnp.sum(
        pick0_ref[...].astype(jnp.float32) * weights_ref[0:1]
        + pick1_ref[...].astype(jnp.float32) * weights_ref[1:2],
        axis=1,
        keepdims=True,
    )
    total = plain(pick0_ref[...] + pick1_ref[...], own) * weight
    pack_rows(total, scratch_ref, packed_ref, slots // shards)


def unpack_kernel(in_ref, top_ref, bottom_ref, scratch_ref):
    half, width = top_ref.shape
    rows = unpack_rows(in_ref, scratch_ref, 2 * half // in_ref.shape[0], width)
    top_ref[...] = rows[:half]
    bottom_ref[...] = rows[half:]


def offsets(place_ref, groups, span):
    return [
        pl.multiple_of(lax.rem(place_ref[0] + k, groups) * span, span) for k in range(groups)
    ]


def pre_kernel(place_ref, *refs):
    *blocks, gate_ref, up_ref, gate_out_ref, up_out_ref = refs
    span = blocks[0].shape[1]
    at = offsets(place_ref, gate_ref.shape[0] // span, span)
    own, right, left = (joined(*blocks[k : k + 2]) for k in (0, 2, 4))
    for w_ref, out_ref in ((gate_ref, gate_out_ref), (up_ref, up_out_ref)):
        total = plain(own, w_ref[pl.ds(at[0], span), :])
        total = total + plain(right, w_ref[pl.ds(at[1], span), :])
        out_ref[...] = total + plain(left, w_ref[pl.ds(at[3], span), :])


def forward_kernel(
    place_ref,
    gate_near_ref,
    up_near_ref,
    top_ref,
    bottom_ref,
    gate_ref,
    up_ref,
    _corner_ref,
    act_ref,
    gate_factor_ref,
    up_factor_ref,
):
    _, span = top_ref.shape
    at = offsets(place_ref, gate_ref.shape[0] // span, span)
    far = joined(top_ref, bottom_ref)
    gate_pre = gate_near_ref[...] + plain(far, gate_ref[pl.ds(at[2], span), :])
    up_pre = up_near_ref[...] + plain(far, up_ref[pl.ds(at[2], span), :])
    gate = jnp.minimum(gate_pre, CLAMP_LIMIT)
    up_one = jnp.clip(up_pre, -CLAMP_LIMIT, CLAMP_LIMIT) + 1.0
    sig = jax.nn.sigmoid(SHARPNESS * gate)
    swish = gate * sig
    act_ref[...] = (up_one * swish).astype(jnp.bfloat16)
    gate_factor_ref[...] = jnp.where(
        gate_pre < CLAMP_LIMIT, up_one * (sig + SHARPNESS * swish * (1.0 - sig)), 0.0
    )
    up_factor_ref[...] = jnp.where(jnp.abs(up_pre) < CLAMP_LIMIT, swish, 0.0)


def near_kernel(place_ref, *refs):
    *blocks, down_ref, total_ref = refs
    span = blocks[0].shape[1]
    at = offsets(place_ref, down_ref.shape[1] // span, span)
    own, right, left = (joined(*blocks[k : k + 2]) for k in (0, 2, 4))
    total = last_dims(own, down_ref[:, pl.ds(at[0], span)])
    total = total + last_dims(right, down_ref[:, pl.ds(at[1], span)])
    total_ref[...] = total + last_dims(left, down_ref[:, pl.ds(at[3], span)])


def delta_kernel(
    place_ref,
    near_ref,
    top_ref,
    bottom_ref,
    down_ref,
    gate_ref,
    up_ref,
    gate_factor_ref,
    up_factor_ref,
    gate_delta_ref,
    up_delta_ref,
    far_top_ref,
    far_bottom_ref,
):
    half, span = top_ref.shape
    at = offsets(place_ref, gate_ref.shape[0] // span, span)
    far = jnp.concatenate([top_ref[...], bottom_ref[...]])
    act_grad = near_ref[...] + last_dims(far, down_ref[:, pl.ds(at[2], span)])
    gate_delta = (act_grad * gate_factor_ref[...]).astype(jnp.bfloat16)
    up_delta = (act_grad * up_factor_ref[...]).astype(jnp.bfloat16)
    gate_delta_ref[...] = gate_delta
    up_delta_ref[...] = up_delta
    out = (
        last_dims(gate_delta, gate_ref[pl.ds(at[2], span), :])
        + last_dims(up_delta, up_ref[pl.ds(at[2], span), :])
    ).astype(jnp.bfloat16)
    far_top_ref[...] = out[:half]
    far_bottom_ref[...] = out[half:]


def partial_kernel(place_ref, gate_delta_ref, up_delta_ref, gate_ref, up_ref, *out_refs):
    span = out_refs[0].shape[1]
    at = offsets(place_ref, gate_ref.shape[0] // span, span)
    for k, ref in zip((1, 3, 0), out_refs):
        ref[...] = last_dims(gate_delta_ref[...], gate_ref[pl.ds(at[k], span), :]) + last_dims(
            up_delta_ref[...], up_ref[pl.ds(at[k], span), :]
        )


def relay_kernel(right_ref, left_ref, from_left_ref, from_right_ref, to_right_ref, to_left_ref):
    half = from_left_ref.shape[0]
    bf = jnp.bfloat16
    to_right_ref[:half] = (right_ref[:half] + from_left_ref[...].astype(jnp.float32)).astype(bf)
    to_right_ref[half:] = right_ref[half:].astype(bf)
    to_left_ref[:half] = left_ref[:half].astype(bf)
    to_left_ref[half:] = (left_ref[half:] + from_right_ref[...].astype(jnp.float32)).astype(bf)


def gather_kernel(own_ref, from_left_ref, from_right_ref, packed_ref, scratch_ref):
    total = (
        own_ref[...]
        + from_left_ref[...].astype(jnp.float32)
        + from_right_ref[...].astype(jnp.float32)
    )
    pack_rows(total, scratch_ref, packed_ref, total.shape[0] // packed_ref.shape[0])


def combine_kernel(in_ref, pick0_ref, pick1_ref, out_ref, scratch_ref):
    pick = pick0_ref[...] + pick1_ref[...]
    rows = unpack_rows(in_ref, scratch_ref, pick.shape[0] // in_ref.shape[0], out_ref.shape[2])
    total = first_dims(pick, rows).astype(jnp.bfloat16)
    for k in range(out_ref.shape[0]):
        out_ref[k] = total


def weights_kernel(place_ref, *refs):
    rows, grads = refs[:8], refs[8:16]
    act_ref, gate_delta_ref, up_delta_ref, gate_out_ref, up_out_ref, down_out_ref = refs[16:]
    span = rows[0].shape[1]
    at = offsets(place_ref, gate_out_ref.shape[0] // span, span)
    bf = jnp.bfloat16
    for k, first in ((0, 0), (1, 2), (3, 4), (2, 6)):
        row = joined(*rows[first : first + 2])
        grad = joined(*grads[first : first + 2])
        gate_out_ref[pl.ds(at[k], span), :] = first_dims(row, gate_delta_ref[...]).astype(bf)
        up_out_ref[pl.ds(at[k], span), :] = first_dims(row, up_delta_ref[...]).astype(bf)
        down_out_ref[:, pl.ds(at[k], span)] = first_dims(act_ref[...], grad).astype(bf)


def on_device(
    mid,
    out_grad,
    expert_ids,
    route_weights,
    gate_proj,
    up_proj,
    down_proj,
    out_proj,
    branch_gate,
    conv_out,
    prior_state,
    rate_gate_w,
    input_gate_w,
    decay_param,
    decay_jump,
    conv_taps,
):
    tok_rows, embedding_width = mid.shape
    shards = lax.axis_size("sp")
    groups = lax.axis_size("tp")
    local_experts = gate_proj.shape[0]
    experts_all = local_experts * shards
    top_count = expert_ids.shape[1]
    expert_room = 3 * top_count * tok_rows // (2 * experts_all)
    slot_count = experts_all * expert_room
    span = embedding_width // groups
    hidden = gate_proj.shape[2]
    bf16, f32 = (jnp.bfloat16, jnp.float32)

    def shaped(*dims, dtype=bf16):
        return jax.ShapeDtypeStruct(dims, dtype)

    vmem = pl.BlockSpec(memory_space=pltpu.VMEM)
    smem = pl.BlockSpec(memory_space=pltpu.SMEM)

    def kernel(body, outs, *args, scalar=None, scratch=(), flops=0):
        lead = () if scalar is None else (scalar,)
        return pl.pallas_call(
            body,
            out_shape=outs,
            in_specs=[smem] * len(lead) + [vmem] * len(args),
            scratch_shapes=list(scratch),
            compiler_params=pltpu.CompilerParams(vmem_limit_bytes=VMEM_ROOM),
            cost_estimate=pl.CostEstimate(flops=flops, transcendentals=0, bytes_accessed=0),
        )(*lead, *args)

    packed_shape = shaped(shards, ROOM_PAD, LANES)
    pack_scratch = pltpu.VMEM((shards * ROOM_PAD, LANES), f32)
    place = lax.axis_index("tp").astype(jnp.int32).reshape(1)
    pick_shape = shaped(slot_count, tok_rows)
    sent_rows, inv_rms, pick0, pick1 = kernel(
        route_kernel,
        (packed_shape, shaped(tok_rows, 1, dtype=f32), pick_shape, pick_shape),
        expert_ids.T,
        mid,
        scalar=place,
        scratch=(pack_scratch,),
    )
    sent_grad = kernel(
        weigh_kernel,
        packed_shape,
        route_weights.T,
        out_grad,
        pick0,
        pick1,
        scalar=place,
        scratch=(pack_scratch,),
        flops=1 << 28,
    )
    heads_local = rate_gate_w.shape[1]
    head_width = rate_gate_w.shape[2]
    channels = heads_local * head_width

    def on_diagonal(w):
        return jnp.concatenate(
            [
                jnp.pad(
                    w[:, h],
                    ((0, 0), (0, 0), (h * head_width, channels - (h + 1) * head_width)),
                )
                for h in range(heads_local)
            ],
            axis=1,
        )

    rate_blocks, input_blocks = on_diagonal(rate_gate_w), on_diagonal(input_gate_w)

    def gate_of(blocks):
        return jax.nn.sigmoid(
            jnp.einsum("stc,scd->std", conv_out, blocks, preferred_element_type=jnp.float32)
        )

    rate_gate, input_gate = gate_of(rate_blocks), gate_of(input_blocks)
    decay_rate = jax.nn.softplus(-decay_param)[:, None, :]
    log_decay = -RATE_SCALE * rate_gate * decay_rate + decay_jump
    decay_factors = jnp.exp(log_decay)
    squared = jnp.exp(2.0 * log_decay)
    norm_factor = jnp.sqrt(STATE_FLOOR - jnp.expm1(2.0 * log_decay))
    conv_full = conv_out.astype(jnp.float32)
    drive_term = input_gate * conv_full
    decayed = decay_factors * prior_state
    states = decayed + norm_factor * drive_term
    summed_states = states[0] + states[1]
    gelu_value, gelu_slope = gelu_parts(branch_gate.astype(jnp.float32))
    mixed_b = (summed_states * gelu_value).astype(jnp.bfloat16)
    rate_coef = (
        (decayed - drive_term * squared / norm_factor)
        * (-RATE_SCALE * decay_rate)
        * rate_gate
        * (1.0 - rate_gate)
    )
    drive_coef = norm_factor * input_gate
    input_coef = norm_factor * conv_full * input_gate * (1.0 - input_gate)
    first_edge = jnp.concatenate([c[0, :EDGE] for c in (drive_coef, rate_coef, input_coef)])
    last_edge = jnp.concatenate([c[1, -EDGE:] for c in (drive_coef, rate_coef, input_coef)])
    (
        sent_grad,
        decay_factors,
        summed_states,
        gelu_value,
        gelu_slope,
        mixed_b,
        rate_coef,
        drive_coef,
        input_coef,
        first_edge,
        last_edge,
    ) = lax.optimization_barrier(
        (
            sent_grad,
            decay_factors,
            summed_states,
            gelu_value,
            gelu_slope,
            mixed_b,
            rate_coef,
            drive_coef,
            input_coef,
            first_edge,
            last_edge,
        )
    )

    half = slot_count // 2

    def unpacked(x):
        return kernel(
            unpack_kernel, (shaped(half, span), shaped(half, span)), x, scratch=(pack_scratch,)
        )

    got_rows = lax.all_to_all(sent_rows, "sp", 0, 0, tiled=True)
    rows, far_rows, corner = ring_blocks(*unpacked(got_rows), "tp")
    got_grad = lax.all_to_all(sent_grad, "sp", 0, 0, tiled=True)
    grads, far_grads, _ = ring_blocks(*unpacked(got_grad), "tp")
    wide_hidden = shaped(slot_count, hidden, dtype=f32)
    gate_near, up_near = kernel(
        pre_kernel,
        (wide_hidden, wide_hidden),
        *rows,
        gate_proj[0],
        up_proj[0],
        scalar=place,
        flops=1 << 30,
    )
    act, gate_factor, up_factor = kernel(
        forward_kernel,
        (shaped(slot_count, hidden), wide_hidden, wide_hidden),
        gate_near,
        up_near,
        *far_rows,
        gate_proj[0],
        up_proj[0],
        corner,
        scalar=place,
        flops=1 << 30,
    )
    forward, backward = ring_pairs("tp")
    near = kernel(near_kernel, wide_hidden, *grads, down_proj[0], scalar=place, flops=1 << 30)
    gate_delta, up_delta, far_top, far_bottom = kernel(
        delta_kernel,
        (
            shaped(slot_count, hidden),
            shaped(slot_count, hidden),
            shaped(half, span),
            shaped(half, span),
        ),
        near,
        *far_grads,
        down_proj[0],
        gate_proj[0],
        up_proj[0],
        gate_factor,
        up_factor,
        scalar=place,
    )
    from_left = lax.ppermute(far_top, "tp", forward)
    from_right = lax.ppermute(far_bottom, "tp", backward)
    part = shaped(slot_count, span, dtype=f32)
    for_right, for_left, for_own = kernel(
        partial_kernel,
        (part, part, part),
        gate_delta,
        up_delta,
        gate_proj[0],
        up_proj[0],
        scalar=place,
        flops=1 << 30,
    )
    to_right, to_left = kernel(
        relay_kernel,
        (shaped(slot_count, span), shaped(slot_count, span)),
        for_right,
        for_left,
        from_left,
        from_right,
    )
    got_left = lax.ppermute(to_right, "tp", forward)
    got_right = lax.ppermute(to_left, "tp", backward)
    summed = kernel(
        gather_kernel, packed_shape, for_own, got_left, got_right, scratch=(pack_scratch,)
    )
    returned = lax.all_to_all(summed, "sp", 0, 0, tiled=True)
    token_copies = kernel(
        combine_kernel,
        shaped(groups, tok_rows, span),
        returned,
        pick0,
        pick1,
        scratch=(pack_scratch,),
    )
    token_grad = lax.all_to_all(token_copies, "tp", 0, 0, tiled=True)
    wide = shaped(2 * tok_rows, channels, dtype=f32)
    edges = shaped(5 * EDGE, channels, dtype=f32)
    piece = embedding_width // shards
    branch_gate_grad, local, prod, sent, low, high = kernel(
        branch_kernel,
        (
            shaped(tok_rows, channels),
            wide,
            wide,
            shaped(shards, piece + 8, channels),
            edges,
            edges,
        ),
        token_grad,
        mid,
        inv_rms,
        out_grad,
        out_proj,
        summed_states,
        gelu_value,
        gelu_slope,
        decay_factors.reshape(2 * tok_rows, channels),
        mixed_b,
        first_edge,
        last_edge,
        scratch=(pltpu.VMEM((tok_rows, channels), f32),),
    )
    ring_on = [(i, i + 1) for i in range(shards - 1)]
    ring_back = [(target, source) for source, target in ring_on]
    got = lax.all_to_all(sent, "sp", 0, 0, tiled=True)
    after = lax.ppermute(low, "sp", ring_back)
    before = lax.ppermute(high, "sp", ring_on)
    gate_grad, up_grad, down_grad = kernel(
        weights_kernel,
        (
            shaped(embedding_width, hidden),
            shaped(embedding_width, hidden),
            shaped(hidden, embedding_width),
        ),
        *rows,
        *far_rows,
        *grads,
        *far_grads,
        act,
        gate_delta,
        up_delta,
        scalar=place,
        flops=1 << 31,
    )
    here = lax.axis_index("sp").astype(jnp.int32).reshape(1)
    input_grad, proj_grad_t = kernel(
        tail_kernel,
        (shaped(tok_rows, channels), shaped(piece, channels, dtype=f32)),
        got,
        local,
        prod,
        drive_coef.reshape(2 * tok_rows, channels),
        rate_coef.reshape(2 * tok_rows, channels),
        input_coef.reshape(2 * tok_rows, channels),
        after,
        before,
        rate_blocks,
        input_blocks,
        conv_taps.astype(f32).reshape(-1, channels),
        scalar=here,
        scratch=[pltpu.VMEM((tok_rows + EDGE, channels), f32)] * 2
        + [pltpu.VMEM((8 * shards, channels), f32)],
    )
    return (
        gate_grad[None],
        up_grad[None],
        down_grad[None],
        proj_grad_t,
        input_grad,
        branch_gate_grad,
    )


def solution(mesh):
    in_specs = (
        P("sp", None),
        P("sp", None),
        P("sp", None),
        P("sp", None),
        P("sp", None, "tp"),
        P("sp", None, "tp"),
        P("sp", "tp", None),
        P("tp", None),
        P("sp", "tp"),
        P(None, "sp", "tp"),
        P(None, "sp", "tp"),
        P(None, "tp", None, None),
        P(None, "tp", None, None),
        P(None, "tp"),
        P(None, "sp", "tp"),
        P(None, None, "tp"),
    )
    out_specs = (
        P("sp", None, "tp"),
        P("sp", None, "tp"),
        P("sp", "tp", None),
        P("sp", "tp"),
        P("sp", "tp"),
        P("sp", "tp"),
    )

    return jax.shard_map(
        on_device, mesh=mesh, in_specs=in_specs, out_specs=out_specs, check_vma=False
    )
```

```python
import jax
import jax.numpy as jnp
from jax import lax
from jax.experimental import pallas as pl
from jax.experimental.pallas import tpu as pltpu
from jax.sharding import PartitionSpec as P

RATE_SCALE = 8.0
CLAMP_LIMIT = 7.0
SHARPNESS = 1.702
NORM_EPSILON = 1e-06
STATE_FLOOR = 0.001
GELU_CUBIC = 0.044715
GELU_SCALE = 0.7978845608028654
LANES = 128


def ring_pairs(axis):
    count = lax.axis_size(axis)
    forward = [(i, (i + 1) % count) for i in range(count)]
    return forward, [(target, source) for source, target in forward]


def ring_blocks(top, bottom, axis):
    forward, backward = ring_pairs(axis)
    left_top = lax.ppermute(top, axis, forward)
    right_bottom = lax.ppermute(bottom, axis, backward)
    left_bottom = lax.ppermute(bottom, axis, forward)
    right_top = lax.ppermute(top, axis, backward)
    far_top = lax.ppermute(left_top, axis, forward)
    far_bottom = lax.ppermute(right_bottom, axis, backward)
    corner = left_top[:8, :LANES] + right_bottom[:8, :LANES]
    near = (top, bottom, right_top, right_bottom, left_top, left_bottom)
    return near, (far_top, far_bottom), corner


def gelu_parts(values):
    inside = GELU_SCALE * (values + GELU_CUBIC * values * values * values)
    tangent = jnp.tanh(inside)
    result = 0.5 * values * (1.0 + tangent)
    slope_value = 0.5 * (1.0 + tangent) + 0.5 * values * (1.0 - tangent * tangent) * GELU_SCALE * (
        1.0 + 3.0 * GELU_CUBIC * values * values
    )
    return (result, slope_value)


SEGMENTS = 8
EDGE = 8


def over_segments(a_rows, b_rows, order):
    carry, factor = jnp.zeros_like(a_rows[:1]), jnp.ones_like(a_rows[:1])
    carries, factors = [None] * SEGMENTS, [None] * SEGMENTS
    for s in order:
        carries[s], factors[s] = carry, factor
        a, b = a_rows[s : s + 1], b_rows[s : s + 1]
        carry, factor = a * carry + b, a * factor
    return jnp.concatenate(carries), jnp.concatenate(factors), factor, carry


def scan_side(seed_ref, decay_ref, local_ref, prod_ref, base, rows, reverse):
    step = rows // SEGMENTS

    def at(i):
        return pl.ds(base + i, SEGMENTS, stride=step)

    order = list(range(step))[::-1] if reverse else list(range(step))
    value = factor = last = None
    for i in order:
        seed = seed_ref[pl.ds(i, SEGMENTS, stride=step), :]
        value = seed if value is None else seed + last * value
        factor = jnp.ones_like(seed) if factor is None else factor * last
        local_ref[at(i), :] = value
        prod_ref[at(i), :] = factor
        last = decay_ref[at(i), :]
    segs = range(SEGMENTS)[::-1] if reverse else range(SEGMENTS)
    carries, factors, whole_factor, whole_value = over_segments(
        factor * last, value * last, segs
    )
    for i in range(step):
        prod = prod_ref[at(i), :]
        local_ref[at(i), :] = local_ref[at(i), :] + prod * carries
        prod_ref[at(i), :] = prod * factors
    return whole_factor, whole_value


def branch_kernel(
    token_ref,
    mid_ref,
    inv_ref,
    cot_ref,
    out_proj_ref,
    states_ref,
    gelu_ref,
    slope_ref,
    decay_ref,
    mixed_ref,
    first_ref,
    last_ref,
    gate_out_ref,
    local_ref,
    prod_ref,
    send_ref,
    low_ref,
    high_ref,
    seed_ref,
):
    shards = send_ref.shape[0]
    share = shards // token_ref.shape[0]
    piece = token_ref.shape[2] // share
    groups, rows, span = token_ref.shape
    inv = inv_ref[...]
    total = jnp.zeros_like(inv)
    for k in range(groups):
        cols = slice(k * span, (k + 1) * span)
        normed = mid_ref[:, cols].astype(jnp.float32) * inv
        total = total + jnp.sum(
            token_ref[k].astype(jnp.float32) * normed, axis=1, keepdims=True
        )
    mean = total / (groups * span)
    branch = jnp.zeros(states_ref.shape, jnp.float32)
    for k in range(groups):
        cols = slice(k * span, (k + 1) * span)
        normed = mid_ref[:, cols].astype(jnp.float32) * inv
        grad = (
            cot_ref[:, cols].astype(jnp.float32)
            + inv * (token_ref[k].astype(jnp.float32) - normed * mean)
        ).astype(jnp.bfloat16)
        branch = branch + last_dims(grad, out_proj_ref[:, cols])
        proj = first_dims(grad, mixed_ref[...]).astype(jnp.bfloat16)
        send_ref[k * share : (k + 1) * share, :piece, :] = proj.reshape(share, piece, LANES)
    gate_out_ref[...] = (branch * states_ref[...] * slope_ref[...]).astype(jnp.bfloat16)
    seed_ref[...] = branch * gelu_ref[...]
    later = scan_side(seed_ref, decay_ref, local_ref, prod_ref, 0, rows, True)
    earlier = scan_side(seed_ref, decay_ref, local_ref, prod_ref, rows, rows, False)
    maps = jnp.concatenate([*later, *earlier])
    high_part = maps.astype(jnp.bfloat16)
    low_part = (maps - high_part.astype(jnp.float32)).astype(jnp.bfloat16)
    pair = jnp.concatenate(
        [high_part.astype(jnp.float32), low_part.astype(jnp.float32)]
    ).astype(jnp.bfloat16)
    send_ref[:, piece:, :] = jnp.broadcast_to(pair[None], (shards, *pair.shape))
    low_ref[:EDGE] = local_ref[:EDGE]
    low_ref[EDGE : 2 * EDGE] = prod_ref[:EDGE]
    low_ref[2 * EDGE :] = first_ref[...]
    high_ref[:EDGE] = local_ref[2 * rows - EDGE :]
    high_ref[EDGE : 2 * EDGE] = prod_ref[2 * rows - EDGE :]
    high_ref[2 * EDGE :] = last_ref[...]


def folded(maps_ref, which, kept, reverse):
    count = maps_ref.shape[0] // 8
    step = count // SEGMENTS
    lead = step * lax.broadcasted_iota(jnp.int32, (SEGMENTS, LANES), 0)
    value = jnp.zeros((SEGMENTS, LANES), jnp.float32)
    factor = jnp.ones((SEGMENTS, LANES), jnp.float32)
    for i in range(step)[::-1] if reverse else range(step):
        use = kept(lead + i)
        a, b = (
            maps_ref[pl.ds(8 * i + q, SEGMENTS, stride=8 * step), :]
            + maps_ref[pl.ds(8 * i + q + 4, SEGMENTS, stride=8 * step), :]
            for q in (which, which + 1)
        )
        a, b = jnp.where(use, a, 1.0), jnp.where(use, b, 0.0)
        value, factor = a * value + b, factor * a
    carry = jnp.zeros((1, LANES), jnp.float32)
    for s in range(SEGMENTS)[::-1] if reverse else range(SEGMENTS):
        carry = factor[s : s + 1] * carry + value[s : s + 1]
    return carry


def tail_kernel(
    here_ref,
    got_ref,
    local_ref,
    prod_ref,
    drive_ref,
    rate_ref,
    input_ref,
    after_ref,
    before_ref,
    rate_w_ref,
    input_w_ref,
    taps_ref,
    out_ref,
    proj_ref,
    later_ref,
    earlier_ref,
    maps_ref,
):
    here = here_ref[0]
    piece = proj_ref.shape[0]
    proj_ref[...] = jnp.sum(got_ref[:, :piece, :].astype(jnp.float32), axis=0)
    maps_ref[...] = got_ref[:, piece:, :].astype(jnp.float32).reshape(maps_ref.shape)
    rows = out_ref.shape[0]
    reach = taps_ref.shape[0] // 2 - 1

    def spread(side, adjoint, drive, rate, inp):
        def back(coef, w_ref):
            return lax.dot_general(
                (adjoint * coef).astype(jnp.bfloat16),
                w_ref[side],
                (((1,), (1,)), ((), ())),
                preferred_element_type=jnp.float32,
            )

        return adjoint * drive + back(rate, rate_w_ref) + back(inp, input_w_ref)

    def main(side, inflow):
        own = slice(side * rows, (side + 1) * rows)
        adjoint = local_ref[own] + prod_ref[own] * inflow
        return spread(side, adjoint, drive_ref[own], rate_ref[own], input_ref[own])

    def edge(side, ref, inflow):
        part = [ref[k * EDGE : (k + 1) * EDGE] for k in range(5)]
        return spread(side, part[0] + part[1] * inflow, *part[2:])

    later_ref[:rows] = main(0, folded(maps_ref, 0, lambda j: j > here, True))
    later_ref[rows:] = edge(0, after_ref, folded(maps_ref, 0, lambda j: j > here + 1, True))
    earlier_ref[:EDGE] = edge(
        1, before_ref, folded(maps_ref, 2, lambda j: j < here - 1, False)
    )
    earlier_ref[EDGE:] = main(1, folded(maps_ref, 2, lambda j: j < here, False))
    total = jnp.zeros((rows, LANES), jnp.float32)
    for k in range(reach + 1):
        up, down = reach - k, EDGE - reach + k
        total = total + taps_ref[k : k + 1] * later_ref[up : up + rows]
        total = (
            total
            + taps_ref[reach + 1 + k : reach + 2 + k] * earlier_ref[down : down + rows]
        )
    out_ref[...] = total.astype(jnp.bfloat16)


ROOM_PAD = 40
VMEM_ROOM = 14 << 20


def row_of(slot, part, parts):
    return slot * parts + part


def pack_rows(value, scratch_ref, out_ref, room):
    shards = out_ref.shape[0]
    parts = value.shape[1] // LANES
    for r in range(room):
        for c in range(parts):
            scratch_ref[pl.ds(row_of(r, c, parts), shards, stride=ROOM_PAD), :] = value[
                r * shards : (r + 1) * shards, c * LANES : (c + 1) * LANES
            ]
    for extra in range(room * parts, ROOM_PAD):
        scratch_ref[pl.ds(extra, shards, stride=ROOM_PAD), :] = jnp.zeros(
            (shards, LANES), jnp.float32
        )
    out_ref[...] = scratch_ref[...].reshape(out_ref.shape).astype(jnp.bfloat16)


def unpack_rows(in_ref, scratch_ref, room, width):
    shards = in_ref.shape[0]
    parts = width // LANES
    scratch_ref[...] = in_ref[...].astype(jnp.float32).reshape(scratch_ref.shape)
    return jnp.concatenate(
        [
            jnp.concatenate(
                [
                    scratch_ref[pl.ds(row_of(r, c, parts), shards, stride=ROOM_PAD), :]
                    for c in range(parts)
                ],
                axis=1,
            )
            for r in range(room)
        ]
    ).astype(jnp.bfloat16)


def joined(top_ref, bottom_ref):
    return jnp.concatenate([top_ref[...], bottom_ref[...]])


def first_dims(a, b):
    return lax.dot_general(a, b, (((0,), (0,)), ((), ())), preferred_element_type=jnp.float32)


def last_dims(a, b):
    return lax.dot_general(a, b, (((1,), (1,)), ((), ())), preferred_element_type=jnp.float32)


def plain(a, b):
    return jnp.dot(a, b, preferred_element_type=jnp.float32)


def route_kernel(
    place_ref,
    ids_hbm,
    mid_hbm,
    packed_ref,
    inv_ref,
    pick0_ref,
    pick1_ref,
    scratch_ref,
    ids_ref,
    mid_ref,
    ids_sem,
    mid_sem,
):
    ids_copy = pltpu.make_async_copy(ids_hbm, ids_ref, ids_sem)
    mid_copy = pltpu.make_async_copy(mid_hbm, mid_ref, mid_sem)
    ids_copy.start()
    mid_copy.start()
    rows, width = mid_ref.shape
    shards = packed_ref.shape[0]
    slots = pick0_ref.shape[0]
    span = packed_ref.shape[1] * LANES // (slots // shards) // LANES * LANES
    ids_copy.wait()
    ids = ids_ref[...]
    experts = lax.broadcasted_iota(jnp.int32, (shards, rows), 0)
    hits = [ids[k : k + 1] == experts for k in range(2)]
    named = (hits[0] | hits[1]).astype(jnp.bfloat16)
    earlier = (
        lax.broadcasted_iota(jnp.int32, (rows, rows), 0)
        < lax.broadcasted_iota(jnp.int32, (rows, rows), 1)
    ).astype(jnp.bfloat16)
    ranks = plain(named, earlier)
    tall = lax.broadcasted_iota(jnp.int32, (slots, rows), 0)
    picks = []
    for k, ref in enumerate((pick0_ref, pick1_ref)):
        rank = jnp.sum(jnp.where(hits[k], ranks, 0.0), axis=0, keepdims=True)
        target = rank.astype(jnp.int32) * shards + ids[k : k + 1]
        pick = (tall == target).astype(jnp.bfloat16)
        ref[...] = pick
        picks.append(pick)
    mid_copy.wait()
    total = jnp.zeros((rows, 1), jnp.float32)
    step = 512
    for c in range(width // step):
        part = mid_ref[:, c * step : (c + 1) * step].astype(jnp.float32)
        total = total + jnp.sum(part * part, axis=1, keepdims=True)
    inv = lax.rsqrt(total / width + NORM_EPSILON)
    inv_ref[...] = inv
    own = mid_ref[:, pl.ds(pl.multiple_of(place_ref[0] * span, LANES), span)]
    normed = (own.astype(jnp.float32) * inv).astype(jnp.bfloat16)
    pack_rows(plain(picks[0] + picks[1], normed), scratch_ref, packed_ref, slots // shards)


def weigh_kernel(place_ref, weights_ref, cot_ref, pick0_ref, pick1_ref, packed_ref, scratch_ref):
    shards = packed_ref.shape[0]
    slots = pick0_ref.shape[0]
    span = packed_ref.shape[1] * LANES // (slots // shards) // LANES * LANES
    own = cot_ref[:, pl.ds(pl.multiple_of(place_ref[0] * span, LANES), span)]
    weight = jnp.sum(
        pick0_ref[...].astype(jnp.float32) * weights_ref[0:1]
        + pick1_ref[...].astype(jnp.float32) * weights_ref[1:2],
        axis=1,
        keepdims=True,
    )
    total = plain(pick0_ref[...] + pick1_ref[...], own) * weight
    pack_rows(total, scratch_ref, packed_ref, slots // shards)


def unpack_kernel(in_ref, top_ref, bottom_ref, scratch_ref):
    half, width = top_ref.shape
    rows = unpack_rows(in_ref, scratch_ref, 2 * half // in_ref.shape[0], width)
    top_ref[...] = rows[:half]
    bottom_ref[...] = rows[half:]


def offsets(place_ref, groups, span):
    return [
        pl.multiple_of(lax.rem(place_ref[0] + k, groups) * span, span) for k in range(groups)
    ]


def pre_kernel(place_ref, *refs):
    *blocks, gate_ref, up_ref, gate_out_ref, up_out_ref = refs
    span = blocks[0].shape[1]
    at = offsets(place_ref, gate_ref.shape[0] // span, span)
    own, right, left = (joined(*blocks[k : k + 2]) for k in (0, 2, 4))
    for w_ref, out_ref in ((gate_ref, gate_out_ref), (up_ref, up_out_ref)):
        total = plain(own, w_ref[pl.ds(at[0], span), :])
        total = total + plain(right, w_ref[pl.ds(at[1], span), :])
        out_ref[...] = total + plain(left, w_ref[pl.ds(at[3], span), :])


def forward_kernel(
    place_ref,
    gate_near_ref,
    up_near_ref,
    top_ref,
    bottom_ref,
    gate_ref,
    up_ref,
    _corner_ref,
    act_ref,
    gate_factor_ref,
    up_factor_ref,
):
    _, span = top_ref.shape
    at = offsets(place_ref, gate_ref.shape[0] // span, span)
    far = joined(top_ref, bottom_ref)
    gate_pre = gate_near_ref[...] + plain(far, gate_ref[pl.ds(at[2], span), :])
    up_pre = up_near_ref[...] + plain(far, up_ref[pl.ds(at[2], span), :])
    gate = jnp.minimum(gate_pre, CLAMP_LIMIT)
    up_one = jnp.clip(up_pre, -CLAMP_LIMIT, CLAMP_LIMIT) + 1.0
    sig = jax.nn.sigmoid(SHARPNESS * gate)
    swish = gate * sig
    act_ref[...] = (up_one * swish).astype(jnp.bfloat16)
    gate_factor_ref[...] = jnp.where(
        gate_pre < CLAMP_LIMIT, up_one * (sig + SHARPNESS * swish * (1.0 - sig)), 0.0
    )
    up_factor_ref[...] = jnp.where(jnp.abs(up_pre) < CLAMP_LIMIT, swish, 0.0)


def near_kernel(place_ref, *refs):
    *blocks, down_ref, total_ref = refs
    span = blocks[0].shape[1]
    at = offsets(place_ref, down_ref.shape[1] // span, span)
    own, right, left = (joined(*blocks[k : k + 2]) for k in (0, 2, 4))
    total = last_dims(own, down_ref[:, pl.ds(at[0], span)])
    total = total + last_dims(right, down_ref[:, pl.ds(at[1], span)])
    total_ref[...] = total + last_dims(left, down_ref[:, pl.ds(at[3], span)])


def delta_kernel(
    place_ref,
    near_ref,
    top_ref,
    bottom_ref,
    down_ref,
    gate_ref,
    up_ref,
    gate_factor_ref,
    up_factor_ref,
    gate_delta_ref,
    up_delta_ref,
    far_top_ref,
    far_bottom_ref,
):
    half, span = top_ref.shape
    at = offsets(place_ref, gate_ref.shape[0] // span, span)
    far = jnp.concatenate([top_ref[...], bottom_ref[...]])
    act_grad = near_ref[...] + last_dims(far, down_ref[:, pl.ds(at[2], span)])
    gate_delta = (act_grad * gate_factor_ref[...]).astype(jnp.bfloat16)
    up_delta = (act_grad * up_factor_ref[...]).astype(jnp.bfloat16)
    gate_delta_ref[...] = gate_delta
    up_delta_ref[...] = up_delta
    out = (
        last_dims(gate_delta, gate_ref[pl.ds(at[2], span), :])
        + last_dims(up_delta, up_ref[pl.ds(at[2], span), :])
    ).astype(jnp.bfloat16)
    far_top_ref[...] = out[:half]
    far_bottom_ref[...] = out[half:]


def partial_kernel(
    place_ref,
    gate_delta_ref,
    up_delta_ref,
    gate_ref,
    up_ref,
    right_top_ref,
    right_bottom_ref,
    left_top_ref,
    left_bottom_ref,
    own_ref,
):
    half, span = right_top_ref.shape
    at = offsets(place_ref, gate_ref.shape[0] // span, span)

    def part(k):
        return last_dims(gate_delta_ref[...], gate_ref[pl.ds(at[k], span), :]) + last_dims(
            up_delta_ref[...], up_ref[pl.ds(at[k], span), :]
        )

    for k, top_ref, bottom_ref in (
        (1, right_top_ref, right_bottom_ref),
        (3, left_top_ref, left_bottom_ref),
    ):
        total = part(k)
        top_ref[...] = total[:half].astype(top_ref.dtype)
        bottom_ref[...] = total[half:].astype(bottom_ref.dtype)
    own_ref[...] = part(0)


def relay_kernel(top_ref, bottom_ref, from_left_ref, from_right_ref, to_right_ref, to_left_ref):
    to_right_ref[...] = (top_ref[...] + from_left_ref[...].astype(jnp.float32)).astype(
        jnp.bfloat16
    )
    to_left_ref[...] = (bottom_ref[...] + from_right_ref[...].astype(jnp.float32)).astype(
        jnp.bfloat16
    )


def gather_kernel(
    own_ref, left_top_ref, left_bottom_ref, right_top_ref, right_bottom_ref, packed_ref, scratch_ref
):
    left = joined(left_top_ref, left_bottom_ref).astype(jnp.float32)
    right = joined(right_top_ref, right_bottom_ref).astype(jnp.float32)
    total = own_ref[...] + left + right
    pack_rows(total, scratch_ref, packed_ref, total.shape[0] // packed_ref.shape[0])


def combine_kernel(in_ref, pick0_ref, pick1_ref, out_ref, scratch_ref):
    pick = pick0_ref[...] + pick1_ref[...]
    rows = unpack_rows(in_ref, scratch_ref, pick.shape[0] // in_ref.shape[0], out_ref.shape[1])
    total = first_dims(pick, rows).astype(jnp.bfloat16)
    out_ref[...] = total


def weights_kernel(place_ref, *refs):
    rows, grads = refs[:8], refs[8:16]
    act_ref, gate_delta_ref, up_delta_ref, gate_out_ref, up_out_ref, down_out_ref = refs[16:]
    span = rows[0].shape[1]
    at = offsets(place_ref, gate_out_ref.shape[0] // span, span)
    bf = jnp.bfloat16
    for k, first in ((0, 0), (1, 2), (3, 4), (2, 6)):
        row = joined(*rows[first : first + 2])
        grad = joined(*grads[first : first + 2])
        gate_out_ref[pl.ds(at[k], span), :] = first_dims(row, gate_delta_ref[...]).astype(bf)
        up_out_ref[pl.ds(at[k], span), :] = first_dims(row, up_delta_ref[...]).astype(bf)
        down_out_ref[:, pl.ds(at[k], span)] = first_dims(act_ref[...], grad).astype(bf)


def on_device(
    mid,
    out_grad,
    expert_ids,
    route_weights,
    gate_proj,
    up_proj,
    down_proj,
    out_proj,
    branch_gate,
    conv_out,
    prior_state,
    rate_gate_w,
    input_gate_w,
    decay_param,
    decay_jump,
    conv_taps,
):
    tok_rows, embedding_width = mid.shape
    shards = lax.axis_size("sp")
    groups = lax.axis_size("tp")
    local_experts = gate_proj.shape[0]
    experts_all = local_experts * shards
    top_count = expert_ids.shape[1]
    expert_room = 3 * top_count * tok_rows // (2 * experts_all)
    slot_count = experts_all * expert_room
    span = embedding_width // groups
    hidden = gate_proj.shape[2]
    bf16, f32 = (jnp.bfloat16, jnp.float32)

    def shaped(*dims, dtype=bf16):
        return jax.ShapeDtypeStruct(dims, dtype)

    vmem = pl.BlockSpec(memory_space=pltpu.VMEM)
    smem = pl.BlockSpec(memory_space=pltpu.SMEM)

    def kernel(body, outs, *args, scalar=None, scratch=(), flops=0, space=vmem):
        lead = () if scalar is None else (scalar,)
        return pl.pallas_call(
            body,
            out_shape=outs,
            in_specs=[smem] * len(lead) + [space] * len(args),
            scratch_shapes=list(scratch),
            compiler_params=pltpu.CompilerParams(vmem_limit_bytes=VMEM_ROOM),
            cost_estimate=pl.CostEstimate(flops=flops, transcendentals=0, bytes_accessed=0),
        )(*lead, *args)

    packed_shape = shaped(shards, ROOM_PAD, LANES)
    pack_scratch = pltpu.VMEM((shards * ROOM_PAD, LANES), f32)
    place = lax.axis_index("tp").astype(jnp.int32).reshape(1)
    pick_shape = shaped(slot_count, tok_rows)
    sent_rows, inv_rms, pick0, pick1 = kernel(
        route_kernel,
        (packed_shape, pltpu.HBM((tok_rows, 1), f32), pick_shape, pick_shape),
        pltpu.with_memory_space_constraint(expert_ids.T, pltpu.HBM),
        pltpu.with_memory_space_constraint(mid, pltpu.HBM),
        scalar=place,
        scratch=(
            pack_scratch,
            pltpu.VMEM((top_count, tok_rows), jnp.int32),
            pltpu.VMEM((tok_rows, embedding_width), bf16),
            pltpu.SemaphoreType.DMA,
            pltpu.SemaphoreType.DMA,
        ),
        space=pl.BlockSpec(memory_space=pltpu.HBM),
    )
    sent_grad = kernel(
        weigh_kernel,
        packed_shape,
        route_weights.T,
        out_grad,
        pick0,
        pick1,
        scalar=place,
        scratch=(pack_scratch,),
        flops=1 << 28,
    )
    heads_local = rate_gate_w.shape[1]
    head_width = rate_gate_w.shape[2]
    channels = heads_local * head_width

    def on_diagonal(w):
        return jnp.concatenate(
            [
                jnp.pad(
                    w[:, h],
                    ((0, 0), (0, 0), (h * head_width, channels - (h + 1) * head_width)),
                )
                for h in range(heads_local)
            ],
            axis=1,
        )

    rate_blocks, input_blocks = on_diagonal(rate_gate_w), on_diagonal(input_gate_w)

    def gate_of(blocks):
        return jax.nn.sigmoid(
            jnp.einsum("stc,scd->std", conv_out, blocks, preferred_element_type=jnp.float32)
        )

    rate_gate, input_gate = gate_of(rate_blocks), gate_of(input_blocks)
    decay_rate = jax.nn.softplus(-decay_param)[:, None, :]
    log_decay = -RATE_SCALE * rate_gate * decay_rate + decay_jump
    decay_factors = jnp.exp(log_decay)
    squared = jnp.exp(2.0 * log_decay)
    norm_factor = jnp.sqrt(STATE_FLOOR - jnp.expm1(2.0 * log_decay))
    conv_full = conv_out.astype(jnp.float32)
    drive_term = input_gate * conv_full
    decayed = decay_factors * prior_state
    states = decayed + norm_factor * drive_term
    summed_states = states[0] + states[1]
    gelu_value, gelu_slope = gelu_parts(branch_gate.astype(jnp.float32))
    mixed_b = (summed_states * gelu_value).astype(jnp.bfloat16)
    rate_coef = (
        (decayed - drive_term * squared / norm_factor)
        * (-RATE_SCALE * decay_rate)
        * rate_gate
        * (1.0 - rate_gate)
    )
    drive_coef = norm_factor * input_gate
    input_coef = norm_factor * conv_full * input_gate * (1.0 - input_gate)
    first_edge = jnp.concatenate([c[0, :EDGE] for c in (drive_coef, rate_coef, input_coef)])
    last_edge = jnp.concatenate([c[1, -EDGE:] for c in (drive_coef, rate_coef, input_coef)])
    (
        sent_grad,
        decay_factors,
        summed_states,
        gelu_value,
        gelu_slope,
        mixed_b,
        rate_coef,
        drive_coef,
        input_coef,
        first_edge,
        last_edge,
    ) = lax.optimization_barrier(
        (
            sent_grad,
            decay_factors,
            summed_states,
            gelu_value,
            gelu_slope,
            mixed_b,
            rate_coef,
            drive_coef,
            input_coef,
            first_edge,
            last_edge,
        )
    )

    half = slot_count // 2

    def unpacked(x):
        return kernel(
            unpack_kernel, (shaped(half, span), shaped(half, span)), x, scratch=(pack_scratch,)
        )

    got_rows = lax.all_to_all(sent_rows, "sp", 0, 0, tiled=True)
    rows, far_rows, corner = ring_blocks(*unpacked(got_rows), "tp")
    got_grad = lax.all_to_all(sent_grad, "sp", 0, 0, tiled=True)
    grads, far_grads, _ = ring_blocks(*unpacked(got_grad), "tp")
    wide_hidden = shaped(slot_count, hidden, dtype=f32)
    gate_near, up_near = kernel(
        pre_kernel,
        (wide_hidden, wide_hidden),
        *rows,
        gate_proj[0],
        up_proj[0],
        scalar=place,
        flops=1 << 30,
    )
    act, gate_factor, up_factor = kernel(
        forward_kernel,
        (shaped(slot_count, hidden), wide_hidden, wide_hidden),
        gate_near,
        up_near,
        *far_rows,
        gate_proj[0],
        up_proj[0],
        corner,
        scalar=place,
        flops=1 << 30,
    )
    forward, backward = ring_pairs("tp")
    near = kernel(near_kernel, wide_hidden, *grads, down_proj[0], scalar=place, flops=1 << 30)
    gate_delta, up_delta, far_top, far_bottom = kernel(
        delta_kernel,
        (
            shaped(slot_count, hidden),
            shaped(slot_count, hidden),
            shaped(half, span),
            shaped(half, span),
        ),
        near,
        *far_grads,
        down_proj[0],
        gate_proj[0],
        up_proj[0],
        gate_factor,
        up_factor,
        scalar=place,
    )
    from_left = lax.ppermute(far_top, "tp", forward)
    from_right = lax.ppermute(far_bottom, "tp", backward)
    part32 = shaped(half, span, dtype=f32)
    part16 = shaped(half, span)
    right_top, right_bottom, left_top, left_bottom, for_own = kernel(
        partial_kernel,
        (part32, part16, part16, part32, shaped(slot_count, span, dtype=f32)),
        gate_delta,
        up_delta,
        gate_proj[0],
        up_proj[0],
        scalar=place,
        flops=1 << 30,
    )
    got_left_bottom = lax.ppermute(right_bottom, "tp", forward)
    got_right_top = lax.ppermute(left_top, "tp", backward)
    to_right, to_left = kernel(
        relay_kernel, (part16, part16), right_top, left_bottom, from_left, from_right
    )
    got_left_top = lax.ppermute(to_right, "tp", forward)
    got_right_bottom = lax.ppermute(to_left, "tp", backward)
    summed = kernel(
        gather_kernel,
        packed_shape,
        for_own,
        got_left_top,
        got_left_bottom,
        got_right_top,
        got_right_bottom,
        scratch=(pack_scratch,),
    )
    returned = lax.all_to_all(summed, "sp", 0, 0, tiled=True)
    token_part = kernel(
        combine_kernel, shaped(tok_rows, span), returned, pick0, pick1, scratch=(pack_scratch,)
    )
    token_grad = lax.all_gather(token_part, "tp", axis=0, tiled=False)
    wide = shaped(2 * tok_rows, channels, dtype=f32)
    edges = shaped(5 * EDGE, channels, dtype=f32)
    piece = embedding_width // shards
    branch_gate_grad, local, prod, sent, low, high = kernel(
        branch_kernel,
        (
            shaped(tok_rows, channels),
            wide,
            wide,
            shaped(shards, piece + 8, channels),
            edges,
            edges,
        ),
        token_grad,
        mid,
        inv_rms,
        out_grad,
        out_proj,
        summed_states,
        gelu_value,
        gelu_slope,
        decay_factors.reshape(2 * tok_rows, channels),
        mixed_b,
        first_edge,
        last_edge,
        scratch=(pltpu.VMEM((tok_rows, channels), f32),),
    )
    ring_on = [(i, i + 1) for i in range(shards - 1)]
    ring_back = [(target, source) for source, target in ring_on]
    got = lax.all_to_all(sent, "sp", 0, 0, tiled=True)
    after = lax.ppermute(low, "sp", ring_back)
    before = lax.ppermute(high, "sp", ring_on)
    gate_grad, up_grad, down_grad = kernel(
        weights_kernel,
        (
            shaped(embedding_width, hidden),
            shaped(embedding_width, hidden),
            shaped(hidden, embedding_width),
        ),
        *rows,
        *far_rows,
        *grads,
        *far_grads,
        act,
        gate_delta,
        up_delta,
        scalar=place,
        flops=1 << 31,
    )
    here = lax.axis_index("sp").astype(jnp.int32).reshape(1)
    input_grad, proj_grad_t = kernel(
        tail_kernel,
        (shaped(tok_rows, channels), shaped(piece, channels, dtype=f32)),
        got,
        local,
        prod,
        drive_coef.reshape(2 * tok_rows, channels),
        rate_coef.reshape(2 * tok_rows, channels),
        input_coef.reshape(2 * tok_rows, channels),
        after,
        before,
        rate_blocks,
        input_blocks,
        conv_taps.astype(f32).reshape(-1, channels),
        scalar=here,
        scratch=[pltpu.VMEM((tok_rows + EDGE, channels), f32)] * 2
        + [pltpu.VMEM((8 * shards, channels), f32)],
    )
    return (
        gate_grad[None],
        up_grad[None],
        down_grad[None],
        proj_grad_t,
        input_grad,
        branch_gate_grad,
    )


def solution(mesh):
    in_specs = (
        P("sp", None),
        P("sp", None),
        P("sp", None),
        P("sp", None),
        P("sp", None, "tp"),
        P("sp", None, "tp"),
        P("sp", "tp", None),
        P("tp", None),
        P("sp", "tp"),
        P(None, "sp", "tp"),
        P(None, "sp", "tp"),
        P(None, "tp", None, None),
        P(None, "tp", None, None),
        P(None, "tp"),
        P(None, "sp", "tp"),
        P(None, None, "tp"),
    )
    out_specs = (
        P("sp", None, "tp"),
        P("sp", None, "tp"),
        P("sp", "tp", None),
        P("sp", "tp"),
        P("sp", "tp"),
        P("sp", "tp"),
    )

    return jax.shard_map(
        on_device, mesh=mesh, in_specs=in_specs, out_specs=out_specs, check_vma=False
    )
```
